128 devices in a mesh: kv: 16 (over z, x), tp: 8 (over y, core).
Axes of the slice: x: 4, y: 4, z: 4, core: 2. Of those that a mesh axis runs over, the one named last changes fastest.
Arguments:
- tokens: bfloat16 [288, 4096], P(None, 'kv'), may hold values from -40 to 40
- norm_gain: float32 [4096], P('kv'), may hold values from 0.1 to 1.9
- query_weight: bfloat16 [4096, 2048], P('kv', 'tp'), may hold values from -0.09375 to 0.09375
- key_weight: bfloat16 [4096, 2048], P('kv', 'tp'), may hold values from -0.09375 to 0.09375
- value_weight: bfloat16 [4096, 2048], P('kv', 'tp'), may hold values from -0.09375 to 0.09375
- gate_weight: bfloat16 [4096, 32], replicated, may hold values from -0.09375 to 0.09375
- gate_bias: float32 [32], replicated, may hold values from -0.5 to 3
- out_weight: bfloat16 [2048, 4096], P('tp', 'kv'), may hold values from -0.125 to 0.125
- cache_keys: bfloat16 [12, 6144, 2048], P(None, 'kv', 'tp'), may hold values from -1000 to 1000
- cache_values: bfloat16 [12, 6144, 2048], P(None, 'kv', 'tp'), may hold values from -6 to 6
- cache_decay: float32 [12, 32, 6144], P(None, 'tp', 'kv'), may hold values from -6144 to 0, as said below
- lengths: int32 [12], replicated, may hold values from 3073 to 6144
- parents: int32 [12, 24], replicated, may hold values from 0 to 23, as said below
Outputs:
- mixed: bfloat16 [288, 4096], P('tp', 'kv')
The draws below stay inside these ranges and needn't reach their ends.
Inputs may be any that keep to these rules, and one draw needn't show every extreme that they name: `cache_decay`: zero at and beyond lengths of the sequence. parents[s, 0] = 0 and parents[s, n] < n for n > 0.
All inputs are finite; a program needn't handle non-finite values.
Results may differ from the reference program's by a relative error of at most 0.014.
The reference program's roundings to bfloat16 on the way count: a program that leaves them out, or rounds other values in their place, can miss the bound.
Values may be sent and summed in bfloat16 or wider, within the bound.
A program may use at most 64 MiB of HBM per device.

```python
import jax
import jax.numpy as jnp
from jax import lax

D = 4096
ATTENTION_HEADS = 32
HEAD_DIM = 64
SEQUENCE_COUNT = 12
PROPS = 24
POS_DEV = 384
ROWS = 288
CACHE_LENGTH = 6144
GROUP_HEADS = 4
N_KV = 16
N_TP = 8


def length_draw(key):
    drawn = jax.random.randint(jax.random.fold_in(key, 11), (SEQUENCE_COUNT,), CACHE_LENGTH // 2 + 1, CACHE_LENGTH + 1).astype(jnp.int32)
    order = jax.random.permutation(jax.random.fold_in(key, 12), SEQUENCE_COUNT)
    drawn = jnp.where(order == 0, CACHE_LENGTH, drawn)
    return drawn.astype(jnp.int32)


def draw_lengths(key, part):
    return length_draw(key)


def draw_parents(key, part):
    nodes = jnp.arange(PROPS, dtype=jnp.int32)
    lowest = jnp.maximum(nodes - 4, 0)
    spread = jnp.maximum(nodes - lowest, 1)
    raw = jax.random.randint(jax.random.fold_in(key, 3), (SEQUENCE_COUNT, PROPS), 0, 1 << 20)
    picked = lowest[None, :] + raw % spread[None, :]
    return jnp.where(nodes[None, :] > 0, picked, 0).astype(jnp.int32)


def draw_tokens(key, part):
    column = jnp.arange(D, dtype=jnp.float32) / D
    jitter = jnp.exp(jax.random.uniform(jax.random.fold_in(key, 1), (D,), jnp.float32, -0.5, 0.5))
    ramp = jnp.exp(jnp.log(0.4) + jnp.log(9.0) * column)
    base = jnp.clip(jax.random.normal(jax.random.fold_in(key, 2), (ROWS, D), jnp.float32), -6.0, 6.0)
    values = base * ramp[None, :] * jitter[None, :]
    return values.astype(jnp.bfloat16)


def draw_cache_keys(key, part):
    shape = (SEQUENCE_COUNT, CACHE_LENGTH, ATTENTION_HEADS * HEAD_DIM)
    base = jnp.clip(jax.random.normal(jax.random.fold_in(key, 1), shape, jnp.float32), -6.0, 6.0)
    return base.astype(jnp.bfloat16)


def draw_cache_decay(key, part):
    lengths = length_draw(key)
    order = jax.random.permutation(jax.random.fold_in(key, 21), ATTENTION_HEADS)
    slow_decay = order < ATTENTION_HEADS // 2
    slow_rate = 0.6 / CACHE_LENGTH * jnp.exp(jax.random.uniform(jax.random.fold_in(key, 22), (ATTENTION_HEADS,), jnp.float32, -0.7, 0.7))
    fast_rate = jnp.exp(-jax.random.uniform(jax.random.fold_in(key, 23), (ATTENTION_HEADS,), jnp.float32, jnp.log(30.0), jnp.log(100.0)))
    rate = jnp.where(slow_decay, slow_rate, fast_rate)
    rough = jnp.exp(jax.random.uniform(jax.random.fold_in(key, 24), (SEQUENCE_COUNT, ATTENTION_HEADS, CACHE_LENGTH), jnp.float32, -0.7, 0.7))
    blocks = jnp.exp(jax.random.uniform(jax.random.fold_in(key, 25), (SEQUENCE_COUNT, ATTENTION_HEADS, CACHE_LENGTH // POS_DEV), jnp.float32, -0.7, 0.7))
    blocks = jnp.repeat(blocks, POS_DEV, axis=2)
    forget_gates = -rate[None, :, None] * rough * blocks
    window_count = jax.random.randint(jax.random.fold_in(key, 26), (SEQUENCE_COUNT, ATTENTION_HEADS, CACHE_LENGTH), 0, CACHE_LENGTH) < 3
    window_length = jax.random.uniform(jax.random.fold_in(key, 27), (SEQUENCE_COUNT, ATTENTION_HEADS, CACHE_LENGTH), jnp.float32, 0.22, 0.69)
    forget_gates = forget_gates - jnp.where(window_count & slow_decay[None, :, None], window_length, 0.0)
    position = jnp.arange(CACHE_LENGTH, dtype=jnp.int32)
    live = position[None, None, :] < lengths[:, None, None]
    forget_gates = jnp.where(live, forget_gates, 0.0)
    running = jnp.cumsum(forget_gates, axis=2)
    return jnp.where(live, running[:, :, -1:] - running, 0.0)


def shard_levels(rng, shape, pieces, least, largest):
    factor_of, own = 1.0, jax.random.fold_in(rng, 6)
    for dim, blocks in pieces:
        steps = jnp.exp(jax.random.uniform(jax.random.fold_in(own, dim), (blocks,), jnp.float32, least / len(pieces), largest / len(pieces)))
        factor_of = factor_of * jnp.repeat(steps, shape[dim] // blocks).reshape([-1 if axis == dim else 1 for axis in range(len(shape))])
    return factor_of


def noise(rng, shape, width, bound, cuts=(), held_as=jnp.bfloat16):
    factor_of = shard_levels(rng, shape, cuts, -0.22, 0.18) if cuts else 1.0
    values = jax.random.normal(rng, shape, jnp.float32) * width * factor_of
    return jnp.minimum(jnp.maximum(values, -bound), bound).astype(held_as)


def setup_inputs(seed: int = 0) -> dict:
    streams_of = jax.random.split(jax.random.key(seed), 14)
    tokens = draw_tokens(jax.random.fold_in(streams_of[13], 71), 0)
    norm_gain = jnp.clip(1.0 + 0.18 * jax.random.normal(streams_of[1], (D,), jnp.float32), 0.1, 1.9)
    query_weight = noise(streams_of[2], (D, ATTENTION_HEADS * HEAD_DIM), D ** -0.5, 0.09375, ((0, 16), (1, 8)))
    key_weight = noise(streams_of[3], (D, ATTENTION_HEADS * HEAD_DIM), D ** -0.5, 0.09375, ((0, 16), (1, 8)))
    value_weight = noise(streams_of[4], (D, ATTENTION_HEADS * HEAD_DIM), D ** -0.5, 0.09375, ((0, 16), (1, 8)))
    gate_weight = noise(streams_of[5], (D, ATTENTION_HEADS), D ** -0.5, 0.09375)
    gate_bias = jnp.clip(jax.random.uniform(streams_of[6], (ATTENTION_HEADS,), jnp.float32, -0.5, 3.0), -0.5, 3.0)
    out_weight = noise(streams_of[7], (ATTENTION_HEADS * HEAD_DIM, D), (ATTENTION_HEADS * HEAD_DIM) ** -0.5, 0.125, ((0, 8), (1, 16)))
    cache_keys = draw_cache_keys(jax.random.fold_in(streams_of[13], 71), 0)
    cache_values = noise(streams_of[9], (SEQUENCE_COUNT, CACHE_LENGTH, ATTENTION_HEADS * HEAD_DIM), 1.0, 6.0, ((1, 16), (2, 8)))
    cache_decay = draw_cache_decay(jax.random.fold_in(streams_of[13], 71), 0)
    lengths = draw_lengths(jax.random.fold_in(streams_of[13], 71), 0)
    parents = draw_parents(jax.random.fold_in(streams_of[13], 71), 0)
    return dict(tokens=tokens, norm_gain=norm_gain, query_weight=query_weight, key_weight=key_weight, value_weight=value_weight, gate_weight=gate_weight, gate_bias=gate_bias, out_weight=out_weight, cache_keys=cache_keys, cache_values=cache_values, cache_decay=cache_decay, lengths=lengths, parents=parents)


def ancestry_of(parents):
    count = parents.shape[1]
    nodes = jnp.arange(count, dtype=jnp.int32)
    link = (parents[:, :, None] == nodes[None, None, :]).astype(jnp.float32)
    link = jnp.maximum(link, jnp.eye(count, dtype=jnp.float32)[None])
    for _ in range(count.bit_length()):
        link = jnp.minimum(jnp.einsum('snm,smk->snk', link, link, precision=lax.Precision.HIGHEST), 1.0)
    return link

def reference(tokens, norm_gain, query_weight, key_weight, value_weight, gate_weight, gate_bias, out_weight, cache_keys, cache_values, cache_decay, lengths, parents):
    scale = HEAD_DIM ** (-0.5)
    xf = tokens.astype(jnp.float32)
    inverse = lax.rsqrt(lax.optimization_barrier(jnp.mean(xf * xf, axis=1, keepdims=True)) + 1e-06)
    normed = (xf * norm_gain).astype(jnp.bfloat16)

    def project(weight):
        return (inverse * jnp.dot(normed, weight, preferred_element_type=jnp.float32)).astype(jnp.bfloat16)
    queries = project(query_weight).astype(jnp.float32).reshape(SEQUENCE_COUNT, PROPS, ATTENTION_HEADS, HEAD_DIM)
    new_keys = project(key_weight).astype(jnp.float32).reshape(SEQUENCE_COUNT, PROPS, ATTENTION_HEADS, HEAD_DIM)
    new_values = project(value_weight).astype(jnp.float32).reshape(SEQUENCE_COUNT, PROPS, ATTENTION_HEADS, HEAD_DIM)
    log_gates = jax.nn.log_sigmoid(inverse * jnp.dot(normed, gate_weight, preferred_element_type=jnp.float32) + gate_bias)
    log_gates = log_gates.reshape(SEQUENCE_COUNT, PROPS, ATTENTION_HEADS)
    ancestry = ancestry_of(parents)
    path = jnp.einsum('snk,skh->snh', ancestry, log_gates, precision=lax.Precision.HIGHEST)

    def cache_block(block):
        start = (block * POS_DEV).astype(jnp.int32)
        keys_blk = lax.dynamic_slice_in_dim(cache_keys, start, POS_DEV, 1).astype(jnp.float32).reshape(SEQUENCE_COUNT, POS_DEV, ATTENTION_HEADS, HEAD_DIM)
        vals_blk = lax.dynamic_slice_in_dim(cache_values, start, POS_DEV, 1).astype(jnp.float32).reshape(SEQUENCE_COUNT, POS_DEV, ATTENTION_HEADS, HEAD_DIM)
        decay_blk = lax.dynamic_slice_in_dim(cache_decay, start, POS_DEV, 2)
        scores = jnp.einsum('snhd,sjhd->snhj', queries, keys_blk) * scale
        scores = scores + path[..., None] + decay_blk[:, None, :, :]
        position = start + jnp.arange(POS_DEV, dtype=jnp.int32)
        live = (position[None, :] < lengths[:, None])[:, None, None, :]
        scores = jnp.where(live, scores, -1e+30)
        top = lax.optimization_barrier(jnp.max(scores, axis=-1))
        weights = jnp.where(live, jnp.exp(scores - top[..., None]), 0.0)
        total = lax.optimization_barrier(jnp.sum(weights, axis=-1))
        rounded = lax.optimization_barrier(weights.astype(jnp.bfloat16)).astype(jnp.float32)
        mix = jnp.einsum('snhj,sjhd->snhd', rounded, vals_blk)
        return (top, total, mix)
    tops, totals, mixes = lax.map(cache_block, jnp.arange(N_KV, dtype=jnp.int32))
    tree_scores = jnp.einsum('snhd,skhd->snhk', queries, new_keys) * scale
    tree_scores = tree_scores + path[..., None] - jnp.swapaxes(path, 1, 2)[:, None, :, :]
    tree_live = ancestry[:, :, None, :] > 0.5
    tree_scores = jnp.where(tree_live, tree_scores, -1e+30)
    tree_top = lax.optimization_barrier(jnp.max(tree_scores, axis=-1))
    tree_weights = jnp.where(tree_live, jnp.exp(tree_scores - tree_top[..., None]), 0.0)
    tree_total = lax.optimization_barrier(jnp.sum(tree_weights, axis=-1))
    tree_rounded = lax.optimization_barrier(tree_weights.astype(jnp.bfloat16)).astype(jnp.float32)
    tree_mix = jnp.einsum('snhk,skhd->snhd', tree_rounded, new_values)
    best = jnp.maximum(lax.optimization_barrier(jnp.max(tops, axis=0)), tree_top)
    factors = jnp.exp(tops - best[None])
    tree_factor = jnp.exp(tree_top - best)
    numer = lax.optimization_barrier(jnp.sum(factors[..., None] * mixes, axis=0)) + tree_factor[..., None] * tree_mix
    denom = lax.optimization_barrier(jnp.sum(factors * totals, axis=0)) + tree_factor * tree_total
    attended = (numer / denom[..., None]).reshape(ROWS, ATTENTION_HEADS * HEAD_DIM).astype(jnp.bfloat16)
    group = GROUP_HEADS * HEAD_DIM
    mixed = jnp.zeros((ROWS, D), jnp.float32)
    for index in range(N_TP):
        part = jnp.dot(attended[:, index * group:(index + 1) * group], out_weight[index * group:(index + 1) * group], preferred_element_type=jnp.float32)
        mixed = mixed + lax.optimization_barrier(part.astype(jnp.bfloat16)).astype(jnp.float32)
    return mixed.astype(jnp.bfloat16)
```

```python
import functools

import jax
import jax.numpy as jnp
from jax import lax
from jax.experimental import pallas as pl
from jax.experimental.pallas import tpu as pltpu
from jax.sharding import PartitionSpec as P

MESH = pl.DeviceIdType.MESH
F32 = jnp.float32
BF16 = jnp.bfloat16
NKV = 16
NTP = 8
SEQS = 12
PROPS = 24
POS = 384
HEADS = 4
HEAD_DIM = 64
COLS = HEADS * HEAD_DIM
ROWS = SEQS * PROPS
OUT_ROWS = ROWS // NTP
LANES = 128
FULL_WIDTH = 4096.0
NEG = -1e30
GROUP = 2


def nt_dot(a, b, precision=None):
    return lax.dot_general(
        a, b, (((1,), (1,)), ((), ())), preferred_element_type=F32, precision=precision
    )


def owner_of(seq):
    return seq + 1 + seq // 4


def spread(columns, lane):
    halves = []
    for pair in range(2):
        halves.append(jnp.where(lane < HEAD_DIM, columns[2 * pair], columns[2 * pair + 1]))
    return jnp.concatenate(halves, axis=1)


def diagonal(stacked, lane):
    halves = []
    for pair in range(2):
        even = stacked[(2 * pair) * PROPS : (2 * pair + 1) * PROPS, pair * LANES : (pair + 1) * LANES]
        odd = stacked[
            (2 * pair + 1) * PROPS : (2 * pair + 2) * PROPS, pair * LANES : (pair + 1) * LANES
        ]
        halves.append(jnp.where(lane < HEAD_DIM, even, odd))
    return jnp.concatenate(halves, axis=1)


def by_head(q, wide):
    parts = [
        jnp.where((wide >= h * HEAD_DIM) & (wide < (h + 1) * HEAD_DIM), q, 0.0)
        for h in range(HEADS)
    ]
    return jnp.concatenate(parts, axis=0)


def in_three(x):
    high = x.astype(BF16).astype(F32)
    rest = x - high
    mid = rest.astype(BF16).astype(F32)
    return high, mid, rest - mid


def kernel(
    tokens,
    gain,
    wq,
    wk,
    wv,
    gw,
    bias,
    wo,
    ckeys,
    cvals,
    cdecay,
    lengths,
    parents,
    out_ref,
    v_tok,
    v_gain,
    v_wq,
    v_wk,
    v_wv,
    v_gw,
    v_wo,
    v_ck,
    v_cv,
    v_cd,
    s_q,
    s_k,
    s_v,
    r_q,
    r_k,
    r_v,
    g_q,
    s_mix,
    r_mix,
    g_att,
    f_term,
    s_term,
    r_term,
    load_sem,
    q_send,
    q_recv,
    k_send,
    k_recv,
    v_send,
    v_recv,
    gq_send,
    gq_recv,
    m_send,
    m_recv,
    a_send,
    a_recv,
    t_send,
    t_recv,
):
    kv = lax.axis_index("kv")
    tp = lax.axis_index("tp")
    mine = jnp.where(kv == 0, 0, kv - 1 - lax.div(jnp.maximum(kv - 1, 0), 5))
    mine = jnp.minimum(mine, SEQS - 1)
    is_owner = lax.rem(kv, 5) != 0

    barrier = pltpu.get_barrier_semaphore()
    for r in range(1, NKV):
        pl.semaphore_signal(
            barrier, inc=1, device_id={"kv": lax.rem(kv + r, NKV)}, device_id_type=MESH
        )
    for r in range(1, NTP):
        pl.semaphore_signal(
            barrier, inc=1, device_id={"tp": lax.rem(tp + r, NTP)}, device_id_type=MESH
        )

    gate_rows = gw.at[pl.ds(pl.multiple_of(kv * 256, 256), 256)]
    loads = [
        pltpu.make_async_copy(src, dst, load_sem.at[n])
        for n, (src, dst) in enumerate(
            [
                (tokens, v_tok),
                (gain, v_gain),
                (wq, v_wq),
                (gate_rows, v_gw),
                (wk, v_wk),
                (wv, v_wv),
                (ckeys, v_ck),
                (cdecay, v_cd),
                (cvals, v_cv),
                (wo, v_wo),
            ]
        )
    ]
    for load in loads:
        load.start()
    l_tok, l_gain, l_wq, l_gw, l_wk, l_wv, l_ck, l_cd, l_cv, l_wo = loads

    lane = lax.broadcasted_iota(jnp.int32, (PROPS, LANES), 1)
    wide = lax.broadcasted_iota(jnp.int32, (PROPS, COLS), 1)

    def exchange(src, dst, send, recv, seq):
        return pltpu.make_async_remote_copy(
            src_ref=src.at[seq],
            dst_ref=dst.at[kv],
            send_sem=send.at[seq],
            recv_sem=recv.at[kv],
            device_id={"kv": owner_of(seq)},
            device_id_type=MESH,
        )

    def to_owners(src, dst, send, recv):
        def step(j, carry):
            seq = lax.rem(mine + j, SEQS)

            @pl.when(owner_of(seq) != kv)
            def _():
                exchange(src, dst, send, recv, seq).start()

            return carry

        lax.fori_loop(0, SEQS, step, 0)

    def sent_to_owners(src, dst, send, recv):
        def step(seq, carry):
            @pl.when(owner_of(seq) != kv)
            def _():
                exchange(src, dst, send, recv, seq).wait_send()

            return carry

        lax.fori_loop(0, SEQS, step, 0)

    def arrived(src, dst, send, recv):
        def step(i, carry):
            @pl.when(i != kv)
            def _():
                pltpu.make_async_remote_copy(
                    src_ref=src.at[0],
                    dst_ref=dst.at[i],
                    send_sem=send.at[0],
                    recv_sem=recv.at[i],
                    device_id={"kv": i},
                    device_id_type=MESH,
                ).wait_recv()

            return carry

        lax.fori_loop(0, NKV, step, 0)

    def gather_copy(buf, send, recv, peer, slot, seq):
        return pltpu.make_async_remote_copy(
            src_ref=buf.at[seq],
            dst_ref=buf.at[seq],
            send_sem=send.at[slot],
            recv_sem=recv.at[seq],
            device_id={"kv": peer},
            device_id_type=MESH,
        )

    def to_all(buf, send, recv):
        def step(r, carry):
            gather_copy(buf, send, recv, lax.rem(kv + r, NKV), r, mine).start()
            return carry

        lax.fori_loop(1, NKV, step, 0)

    def sent_to_all(buf, send, recv):
        def step(r, carry):
            gather_copy(buf, send, recv, lax.rem(kv + r, NKV), r, mine).wait_send()
            return carry

        lax.fori_loop(1, NKV, step, 0)

    def await_seq(buf, send, recv, seq):
        @pl.when(owner_of(seq) != kv)
        def _():
            gather_copy(buf, send, recv, owner_of(seq), 0, seq).wait_recv()

    l_tok.wait()
    l_gain.wait()
    x = v_tok[...].astype(F32)
    squares = jnp.sum(x * x, axis=1, keepdims=True)
    normed = (x * v_gain[...]).astype(BF16)
    l_wq.wait()
    s_q[:, :, 0:COLS] = jnp.dot(normed, v_wq[...], preferred_element_type=F32).reshape(
        SEQS, PROPS, COLS
    )
    l_gw.wait()
    pick = lax.broadcasted_iota(jnp.int32, (32, LANES), 0) == (
        tp * HEADS + lax.broadcasted_iota(jnp.int32, (32, LANES), 1)
    )
    pick = pick & (lax.broadcasted_iota(jnp.int32, (32, LANES), 1) < HEADS)
    own_gates = jnp.dot(
        v_gw[...], pick.astype(F32).astype(BF16), preferred_element_type=F32
    ).astype(BF16)
    extra = jnp.dot(normed, own_gates, preferred_element_type=F32)
    lane_rows = lax.broadcasted_iota(jnp.int32, (ROWS, LANES), 1)
    extra = jnp.where(lane_rows < HEADS, extra, squares)
    s_q[:, :, COLS:] = extra.reshape(SEQS, PROPS, LANES)

    pl.semaphore_wait(barrier, NKV - 1 + NTP - 1)
    to_owners(s_q, r_q, q_send, q_recv)

    l_wk.wait()
    s_k[...] = jnp.dot(normed, v_wk[...], preferred_element_type=F32).reshape(SEQS, PROPS, COLS)
    to_owners(s_k, r_k, k_send, k_recv)
    l_wv.wait()
    s_v[...] = jnp.dot(normed, v_wv[...], preferred_element_type=F32).reshape(SEQS, PROPS, COLS)

    @pl.when(is_owner)
    def _():
        r_q[kv] = s_q[mine]
        arrived(s_q, r_q, q_send, q_recv)
        total = r_q[0]
        for i in range(1, NKV):
            total = total + r_q[i]
        s_q[mine] = total
        inverse = lax.rsqrt(total[:, COLS + HEADS : COLS + HEADS + 1] / FULL_WIDTH + 1e-6)
        g_q[mine] = (inverse * total[:, :COLS]).astype(BF16)
        to_all(g_q, gq_send, gq_recv)

    to_owners(s_v, r_v, v_send, v_recv)

    l_ck.wait()
    l_cd.wait()
    l_cv.wait()
    position = kv * POS + lax.broadcasted_iota(jnp.int32, (1, POS), 1)

    def attend(seq):
        q = by_head(g_q[seq].astype(F32) * (HEAD_DIM**-0.5), wide).astype(BF16)
        scores = nt_dot(q, v_ck[seq])
        live = position < lengths[seq]
        parts = []
        for h in range(HEADS):
            decay = jnp.where(live, v_cd[seq, h : h + 1, :], NEG)
            parts.append(scores[h * PROPS : (h + 1) * PROPS] + decay)
        scores = jnp.concatenate(parts, axis=0)
        top = jnp.max(scores, axis=1, keepdims=True)
        weights = jnp.exp(scores - top)
        total = jnp.sum(weights, axis=1, keepdims=True)
        mix = jnp.dot(weights.astype(BF16), v_cv[seq], preferred_element_type=F32)
        stats = jnp.zeros((PROPS, LANES), F32)
        for h in range(HEADS):
            rows = slice(h * PROPS, (h + 1) * PROPS)
            for n, piece in enumerate(in_three(top[rows]) + in_three(total[rows])):
                stats = jnp.where(lane == n * HEADS + h, piece, stats)
        s_mix[seq] = jnp.concatenate([diagonal(mix, lane), stats], axis=1).astype(BF16)

    def attend_group(j, carry):
        seqs = [lax.rem(mine + j * GROUP + u, SEQS) for u in range(GROUP)]
        for seq in seqs:
            await_seq(g_q, gq_send, gq_recv, seq)
        for seq in seqs:
            attend(seq)
        for seq in seqs:

            @pl.when(owner_of(seq) != kv)
            def _():
                exchange(s_mix, r_mix, m_send, m_recv, seq).start()

        return carry

    lax.fori_loop(0, SEQS // GROUP, attend_group, 0)

    @pl.when(is_owner)
    def _():
        r_k[kv] = s_k[mine]
        r_v[kv] = s_v[mine]
        r_mix[kv] = s_mix[mine]
        summed = s_q[mine]
        inverse = lax.rsqrt(summed[:, COLS + HEADS : COLS + HEADS + 1] / FULL_WIDTH + 1e-6)
        gates = inverse * summed[:, COLS:]
        shift = jnp.zeros((PROPS, LANES), F32)
        for h in range(HEADS):
            shift = jnp.where(lane == h, bias[tp * HEADS + h], shift)
        gates = gates + shift
        log_gates = jnp.minimum(gates, 0.0) - jnp.log1p(jnp.exp(-jnp.abs(gates)))
        square = (PROPS, PROPS)
        older = lax.broadcasted_iota(jnp.int32, square, 0)
        younger = lax.broadcasted_iota(jnp.int32, square, 1)
        linked = (older == parents[pl.ds(mine, 1), :]) | (older == younger)
        up = linked.astype(F32)
        for _ in range(5):
            closed = up.astype(BF16)
            up = jnp.minimum(jnp.dot(closed, closed, preferred_element_type=F32), 1.0)
        eye = (older == younger).astype(F32)
        ancestry = nt_dot(eye.astype(BF16), up.astype(BF16))
        path = jnp.dot(
            ancestry, log_gates, preferred_element_type=F32, precision=lax.Precision.HIGHEST
        )
        padded = jnp.concatenate([path, jnp.zeros((LANES - PROPS, LANES), F32)], axis=0)
        path_rows = padded.T

        arrived(s_k, r_k, k_send, k_recv)
        new_keys = r_k[0]
        for i in range(1, NKV):
            new_keys = new_keys + r_k[i]
        new_keys = (inverse * new_keys).astype(BF16)
        q = by_head(g_q[mine].astype(F32) * (HEAD_DIM**-0.5), wide).astype(BF16)
        scores = nt_dot(q, new_keys)
        parts = []
        for h in range(HEADS):
            part = scores[h * PROPS : (h + 1) * PROPS] - path_rows[h : h + 1, :PROPS]
            parts.append(jnp.where(ancestry > 0.5, part, NEG))
        scores = jnp.concatenate(parts, axis=0)
        tree_top = jnp.max(scores, axis=1, keepdims=True)
        weights = jnp.exp(scores - tree_top)
        tree_total = jnp.sum(weights, axis=1, keepdims=True)
        arrived(s_v, r_v, v_send, v_recv)
        new_values = r_v[0]
        for i in range(1, NKV):
            new_values = new_values + r_v[i]
        new_values = (inverse * new_values).astype(BF16)
        tree_mix = diagonal(
            jnp.dot(weights.astype(BF16), new_values, preferred_element_type=F32), lane
        )
        tree_stats = jnp.zeros((PROPS, LANES), F32)
        for h in range(HEADS):
            rows = slice(h * PROPS, (h + 1) * PROPS)
            tree_stats = jnp.where(lane == h, tree_top[rows], tree_stats)
            tree_stats = jnp.where(lane == 3 * HEADS + h, tree_total[rows], tree_stats)

        arrived(s_mix, r_mix, m_send, m_recv)

        def stats_of(i):
            packed = r_mix[i, :, COLS:].astype(F32)
            one = pltpu.roll(packed, LANES - HEADS, 1)
            two = pltpu.roll(packed, LANES - 2 * HEADS, 1)
            return packed + (one + two)

        stats = [stats_of(i) for i in range(NKV)] + [tree_stats]
        best = functools.reduce(jnp.maximum, stats)
        factors = [jnp.exp(s - best) for s in stats]
        denominator = functools.reduce(
            jnp.add,
            [pltpu.roll(s, LANES - 3 * HEADS, 1) * f for s, f in zip(stats, factors)],
        )
        numerator = jnp.zeros((PROPS, COLS), F32)
        for i in range(NKV + 1):
            values = r_mix[i, :, :COLS].astype(F32) if i < NKV else tree_mix
            numerator = numerator + values * spread(
                [factors[i][:, h : h + 1] for h in range(HEADS)], lane
            )
        below = spread([denominator[:, h : h + 1] for h in range(HEADS)], lane)
        g_att[mine] = (numerator / below).astype(BF16)
        to_all(g_att, a_send, a_recv)

    l_wo.wait()

    def await_attended(seq, carry):
        await_seq(g_att, a_send, a_recv, seq)
        return carry

    lax.fori_loop(0, SEQS, await_attended, 0)
    attended = jnp.concatenate([g_att[s].astype(F32) for s in range(SEQS)], axis=0).astype(BF16)
    f_term[...] = jnp.dot(attended, v_wo[...], preferred_element_type=F32)

    def term_copy(to):
        return pltpu.make_async_remote_copy(
            src_ref=s_term.at[to],
            dst_ref=r_term.at[tp],
            send_sem=t_send.at[to],
            recv_sem=t_recv.at[tp],
            device_id={"tp": to},
            device_id_type=MESH,
        )

    for t in range(NTP):
        s_term[t] = f_term[t * OUT_ROWS : (t + 1) * OUT_ROWS, :].astype(BF16)

    def send_term(r, carry):
        term_copy(lax.rem(tp + r, NTP)).start()
        return carry

    lax.fori_loop(1, NTP, send_term, 0)
    r_term[tp] = s_term[tp]

    def term_arrived(r, carry):
        source = lax.rem(tp + r, NTP)
        pltpu.make_async_remote_copy(
            src_ref=s_term.at[source],
            dst_ref=r_term.at[source],
            send_sem=t_send.at[source],
            recv_sem=t_recv.at[source],
            device_id={"tp": source},
            device_id_type=MESH,
        ).wait_recv()
        return carry

    lax.fori_loop(1, NTP, term_arrived, 0)
    mixed = r_term[0].astype(F32)
    for t in range(1, NTP):
        mixed = mixed + r_term[t].astype(F32)
    out_ref[...] = mixed.astype(BF16)

    sent_to_owners(s_q, r_q, q_send, q_recv)
    sent_to_owners(s_k, r_k, k_send, k_recv)
    sent_to_owners(s_v, r_v, v_send, v_recv)
    sent_to_owners(s_mix, r_mix, m_send, m_recv)

    @pl.when(is_owner)
    def _():
        sent_to_all(g_q, gq_send, gq_recv)
        sent_to_all(g_att, a_send, a_recv)

    def term_sent(r, carry):
        term_copy(lax.rem(tp + r, NTP)).wait_send()
        return carry

    lax.fori_loop(1, NTP, term_sent, 0)


def body(
    tokens,
    norm_gain,
    query_weight,
    key_weight,
    value_weight,
    gate_weight,
    gate_bias,
    out_weight,
    cache_keys,
    cache_values,
    cache_decay,
    lengths,
    parents,
):
    anywhere = pl.BlockSpec(memory_space=pl.ANY)
    scalars = pl.BlockSpec(memory_space=pltpu.SMEM)
    vector = pl.BlockSpec(memory_space=pltpu.VMEM)
    dma = pltpu.SemaphoreType.DMA
    return pl.pallas_call(
        kernel,
        out_shape=jax.ShapeDtypeStruct((OUT_ROWS, COLS), BF16),
        in_specs=[anywhere] * 6 + [scalars] + [anywhere] * 4 + [scalars, vector],
        out_specs=vector,
        scratch_shapes=[
            pltpu.VMEM((ROWS, COLS), BF16),
            pltpu.VMEM((1, COLS), F32),
            pltpu.VMEM((COLS, COLS), BF16),
            pltpu.VMEM((COLS, COLS), BF16),
            pltpu.VMEM((COLS, COLS), BF16),
            pltpu.VMEM((COLS, 32), BF16),
            pltpu.VMEM((COLS, COLS), BF16),
            pltpu.VMEM((SEQS, POS, COLS), BF16),
            pltpu.VMEM((SEQS, POS, COLS), BF16),
            pltpu.VMEM((SEQS, HEADS, POS), F32),
            pltpu.VMEM((SEQS, PROPS, COLS + LANES), F32),
            pltpu.VMEM((SEQS, PROPS, COLS), F32),
            pltpu.VMEM((SEQS, PROPS, COLS), F32),
            pltpu.VMEM((NKV, PROPS, COLS + LANES), F32),
            pltpu.VMEM((NKV, PROPS, COLS), F32),
            pltpu.VMEM((NKV, PROPS, COLS), F32),
            pltpu.VMEM((SEQS, PROPS, COLS), BF16),
            pltpu.VMEM((SEQS, PROPS, COLS + LANES), BF16),
            pltpu.VMEM((NKV, PROPS, COLS + LANES), BF16),
            pltpu.VMEM((SEQS, PROPS, COLS), BF16),
            pltpu.VMEM((ROWS, COLS), F32),
            pltpu.VMEM((NTP, OUT_ROWS, COLS), BF16),
            pltpu.VMEM((NTP, OUT_ROWS, COLS), BF16),
            dma((10,)),
            dma((SEQS,)),
            dma((NKV,)),
            dma((SEQS,)),
            dma((NKV,)),
            dma((SEQS,)),
            dma((NKV,)),
            dma((NKV,)),
            dma((SEQS,)),
            dma((SEQS,)),
            dma((NKV,)),
            dma((NKV,)),
            dma((SEQS,)),
            dma((NTP,)),
            dma((NTP,)),
        ],
        compiler_params=pltpu.CompilerParams(
            collective_id=0, has_side_effects=True, vmem_limit_bytes=60 * 1024 * 1024
        ),
        name="tree_attention",
    )(
        tokens,
        norm_gain.reshape(1, -1),
        query_weight,
        key_weight,
        value_weight,
        gate_weight,
        gate_bias,
        out_weight,
        cache_keys,
        cache_values,
        cache_decay,
        lengths,
        parents,
    )


def solution(mesh):
    in_specs = (
        P(None, "kv"),
        P("kv"),
        P("kv", "tp"),
        P("kv", "tp"),
        P("kv", "tp"),
        P(),
        P(),
        P("tp", "kv"),
        P(None, "kv", "tp"),
        P(None, "kv", "tp"),
        P(None, "tp", "kv"),
        P(),
        P(),
    )
    out_specs = P("tp", "kv")
    return jax.shard_map(body, mesh=mesh, in_specs=in_specs, out_specs=out_specs, check_vma=False)
```

```python
import functools

import jax
import jax.numpy as jnp
from jax import lax
from jax.experimental import pallas as pl
from jax.experimental.pallas import tpu as pltpu
from jax.sharding import PartitionSpec as P

MESH = pl.DeviceIdType.MESH
F32 = jnp.float32
BF16 = jnp.bfloat16
NKV = 16
NTP = 8
SEQS = 12
PROPS = 24
POS = 384
HEADS = 4
HEAD_DIM = 64
COLS = HEADS * HEAD_DIM
ROWS = SEQS * PROPS
OUT_ROWS = ROWS // NTP
LANES = 128
FULL_WIDTH = 4096.0
NEG = -1e30
GROUP = 3


def nt_dot(a, b, precision=None):
    return lax.dot_general(
        a, b, (((1,), (1,)), ((), ())), preferred_element_type=F32, precision=precision
    )


def owner_of(seq):
    return seq + 1 + seq // 4


def spread(columns, lane):
    halves = []
    for pair in range(2):
        halves.append(jnp.where(lane < HEAD_DIM, columns[2 * pair], columns[2 * pair + 1]))
    return jnp.concatenate(halves, axis=1)


def diagonal(stacked, lane):
    halves = []
    for pair in range(2):
        even = stacked[(2 * pair) * PROPS : (2 * pair + 1) * PROPS, pair * LANES : (pair + 1) * LANES]
        odd = stacked[
            (2 * pair + 1) * PROPS : (2 * pair + 2) * PROPS, pair * LANES : (pair + 1) * LANES
        ]
        halves.append(jnp.where(lane < HEAD_DIM, even, odd))
    return jnp.concatenate(halves, axis=1)


def by_head(q, wide):
    parts = [
        jnp.where((wide >= h * HEAD_DIM) & (wide < (h + 1) * HEAD_DIM), q, 0.0)
        for h in range(HEADS)
    ]
    return jnp.concatenate(parts, axis=0)


def in_three(x):
    high = x.astype(BF16).astype(F32)
    rest = x - high
    mid = rest.astype(BF16).astype(F32)
    return high, mid, rest - mid


def kernel(
    tokens,
    gain,
    wq,
    wk,
    wv,
    gw,
    bias,
    wo,
    ckeys,
    cvals,
    cdecay,
    lengths,
    parents,
    out_ref,
    v_tok,
    v_gain,
    v_wq,
    v_wk,
    v_wv,
    v_gw,
    v_wo,
    v_ck,
    v_cv,
    v_cd,
    s_q,
    s_k,
    s_v,
    r_q,
    r_k,
    r_v,
    g_q,
    s_mix,
    r_mix,
    g_att,
    f_term,
    s_term,
    load_sem,
    q_send,
    q_recv,
    k_send,
    k_recv,
    v_send,
    v_recv,
    gq_send,
    gq_recv,
    m_send,
    m_recv,
    a_send,
    a_recv,
    t_send,
    t_recv,
):
    kv = lax.axis_index("kv")
    tp = lax.axis_index("tp")
    mine = jnp.where(kv == 0, 0, kv - 1 - lax.div(jnp.maximum(kv - 1, 0), 5))
    mine = jnp.minimum(mine, SEQS - 1)
    is_owner = lax.rem(kv, 5) != 0

    barrier = pltpu.get_barrier_semaphore()
    for r in range(1, NKV):
        pl.semaphore_signal(
            barrier, inc=1, device_id={"kv": lax.rem(kv + r, NKV)}, device_id_type=MESH
        )
    for r in range(1, NTP):
        pl.semaphore_signal(
            barrier, inc=1, device_id={"tp": lax.rem(tp + r, NTP)}, device_id_type=MESH
        )

    gate_cols = gw.at[:, pl.ds(pl.multiple_of(kv * COLS, COLS), COLS)]
    loads = [
        pltpu.make_async_copy(src, dst, load_sem.at[n])
        for n, (src, dst) in enumerate(
            [
                (tokens, v_tok),
                (gain, v_gain),
                (wq, v_wq),
                (gate_cols, v_gw),
                (wk, v_wk),
                (wv, v_wv),
                (ckeys, v_ck),
                (cdecay, v_cd),
                (cvals, v_cv),
                (wo, v_wo),
            ]
        )
    ]
    for load in loads:
        load.start()
    l_tok, l_gain, l_wq, l_gw, l_wk, l_wv, l_ck, l_cd, l_cv, l_wo = loads

    lane = lax.broadcasted_iota(jnp.int32, (PROPS, LANES), 1)
    wide = lax.broadcasted_iota(jnp.int32, (PROPS, COLS), 1)

    def exchange(src, dst, send, recv, seq):
        return pltpu.make_async_remote_copy(
            src_ref=src.at[seq],
            dst_ref=dst.at[kv],
            send_sem=send.at[seq],
            recv_sem=recv.at[kv],
            device_id={"kv": owner_of(seq)},
            device_id_type=MESH,
        )

    def to_owners(src, dst, send, recv):
        def step(j, carry):
            seq = lax.rem(mine + j, SEQS)

            @pl.when(owner_of(seq) != kv)
            def _():
                exchange(src, dst, send, recv, seq).start()

            return carry

        lax.fori_loop(0, SEQS, step, 0)

    def sent_to_owners(src, dst, send, recv):
        def step(seq, carry):
            @pl.when(owner_of(seq) != kv)
            def _():
                exchange(src, dst, send, recv, seq).wait_send()

            return carry

        lax.fori_loop(0, SEQS, step, 0)

    def arrived(src, dst, send, recv):
        def step(i, carry):
            @pl.when(i != kv)
            def _():
                pltpu.make_async_remote_copy(
                    src_ref=src.at[0],
                    dst_ref=dst.at[i],
                    send_sem=send.at[0],
                    recv_sem=recv.at[i],
                    device_id={"kv": i},
                    device_id_type=MESH,
                ).wait_recv()

            return carry

        lax.fori_loop(0, NKV, step, 0)

    def gather_copy(buf, send, recv, peer, slot, seq):
        return pltpu.make_async_remote_copy(
            src_ref=buf.at[seq],
            dst_ref=buf.at[seq],
            send_sem=send.at[slot],
            recv_sem=recv.at[seq],
            device_id={"kv": peer},
            device_id_type=MESH,
        )

    def to_all(buf, send, recv):
        def step(r, carry):
            gather_copy(buf, send, recv, lax.rem(kv + r, NKV), r, mine).start()
            return carry

        lax.fori_loop(1, NKV, step, 0)

    def sent_to_all(buf, send, recv):
        def step(r, carry):
            gather_copy(buf, send, recv, lax.rem(kv + r, NKV), r, mine).wait_send()
            return carry

        lax.fori_loop(1, NKV, step, 0)

    def await_seq(buf, send, recv, seq):
        @pl.when(owner_of(seq) != kv)
        def _():
            gather_copy(buf, send, recv, owner_of(seq), 0, seq).wait_recv()

    pending = []

    l_tok.wait()
    l_gain.wait()
    x = v_tok[...].astype(F32)
    squares = jnp.sum(x * x, axis=1, keepdims=True)
    normed = (x * v_gain[...]).astype(BF16)
    l_wq.wait()
    s_q[:, :, 0:COLS] = jnp.dot(normed, v_wq[...], preferred_element_type=F32).reshape(
        SEQS, PROPS, COLS
    )
    l_gw.wait()
    pick_row = lax.broadcasted_iota(jnp.int32, (LANES, 32), 0)
    pick_col = lax.broadcasted_iota(jnp.int32, (LANES, 32), 1)
    pick = (pick_col == tp * HEADS + pick_row) & (pick_row < HEADS)
    own_gates = jnp.dot(
        pick.astype(F32).astype(BF16), v_gw[...], preferred_element_type=F32
    ).astype(BF16)
    extra = nt_dot(normed, own_gates)
    lane_rows = lax.broadcasted_iota(jnp.int32, (ROWS, LANES), 1)
    extra = jnp.where(lane_rows < HEADS, extra, squares)
    s_q[:, :, COLS:] = extra.reshape(SEQS, PROPS, LANES)

    pl.semaphore_wait(barrier, NKV - 1 + NTP - 1)
    to_owners(s_q, r_q, q_send, q_recv)
    pending.append(lambda: sent_to_owners(s_q, r_q, q_send, q_recv))

    l_wk.wait()
    s_k[...] = jnp.dot(normed, v_wk[...], preferred_element_type=F32).reshape(SEQS, PROPS, COLS)
    l_wv.wait()
    new = jnp.dot(normed, v_wv[...], preferred_element_type=F32)
    s_v[...] = new.astype(BF16).reshape(SEQS, PROPS, COLS)

    @pl.when(is_owner)
    def _():
        r_q[kv] = s_q[mine]
        arrived(s_q, r_q, q_send, q_recv)
        total = r_q[0]
        for i in range(1, NKV):
            total = total + r_q[i]
        s_q[mine] = total
        inverse = lax.rsqrt(total[:, COLS + HEADS : COLS + HEADS + 1] / FULL_WIDTH + 1e-6)
        g_q[mine] = (inverse * total[:, :COLS]).astype(BF16)
        to_all(g_q, gq_send, gq_recv)

    pending.append(lambda: pl.when(is_owner)(lambda: sent_to_all(g_q, gq_send, gq_recv)))
    to_owners(s_k, r_k, k_send, k_recv)
    pending.append(lambda: sent_to_owners(s_k, r_k, k_send, k_recv))
    to_owners(s_v, r_v, v_send, v_recv)
    pending.append(lambda: sent_to_owners(s_v, r_v, v_send, v_recv))

    l_ck.wait()
    l_cd.wait()
    l_cv.wait()
    position = kv * POS + lax.broadcasted_iota(jnp.int32, (1, POS), 1)

    def attend(seq):
        q = by_head(g_q[seq].astype(F32) * (HEAD_DIM**-0.5), wide).astype(BF16)
        scores = nt_dot(q, v_ck[seq])
        live = position < lengths[seq]
        parts = []
        for h in range(HEADS):
            decay = jnp.where(live, v_cd[seq, h : h + 1, :], NEG)
            parts.append(scores[h * PROPS : (h + 1) * PROPS] + decay)
        scores = jnp.concatenate(parts, axis=0)
        top = jnp.max(scores, axis=1, keepdims=True)
        weights = jnp.exp(scores - top)
        total = jnp.sum(weights, axis=1, keepdims=True)
        mix = jnp.dot(weights.astype(BF16), v_cv[seq], preferred_element_type=F32)
        stats = jnp.zeros((PROPS, LANES), F32)
        for h in range(HEADS):
            rows = slice(h * PROPS, (h + 1) * PROPS)
            for n, piece in enumerate(in_three(top[rows]) + in_three(total[rows])):
                stats = jnp.where(lane == n * HEADS + h, piece, stats)
        s_mix[seq] = jnp.concatenate([diagonal(mix, lane), stats], axis=1).astype(BF16)

    def attend_group(j, carry):
        seqs = [lax.rem(mine + SEQS - j * GROUP - u, SEQS) for u in range(GROUP)]
        for seq in seqs:
            await_seq(g_q, gq_send, gq_recv, seq)
        for seq in seqs:
            attend(seq)
        for seq in seqs:

            @pl.when(owner_of(seq) != kv)
            def _():
                exchange(s_mix, r_mix, m_send, m_recv, seq).start()

        return carry

    lax.fori_loop(0, SEQS // GROUP, attend_group, 0)

    pending.append(lambda: sent_to_owners(s_mix, r_mix, m_send, m_recv))
    @pl.when(is_owner)
    def _():
        r_k[kv] = s_k[mine]
        r_v[kv] = s_v[mine]
        r_mix[kv] = s_mix[mine]
        summed = s_q[mine]
        inverse = lax.rsqrt(summed[:, COLS + HEADS : COLS + HEADS + 1] / FULL_WIDTH + 1e-6)
        gates = inverse * summed[:, COLS:]
        shift = jnp.zeros((PROPS, LANES), F32)
        for h in range(HEADS):
            shift = jnp.where(lane == h, bias[tp * HEADS + h], shift)
        gates = gates + shift
        log_gates = jnp.minimum(gates, 0.0) - jnp.log1p(jnp.exp(-jnp.abs(gates)))
        square = (PROPS, PROPS)
        older = lax.broadcasted_iota(jnp.int32, square, 0)
        younger = lax.broadcasted_iota(jnp.int32, square, 1)
        linked = (older == parents[pl.ds(mine, 1), :]) | (older == younger)
        up = linked.astype(F32)
        for _ in range(5):
            closed = up.astype(BF16)
            up = jnp.minimum(jnp.dot(closed, closed, preferred_element_type=F32), 1.0)
        eye = (older == younger).astype(F32)
        ancestry = nt_dot(eye.astype(BF16), up.astype(BF16))
        path = jnp.dot(
            ancestry, log_gates, preferred_element_type=F32, precision=lax.Precision.HIGHEST
        )
        padded = jnp.concatenate([path, jnp.zeros((LANES - PROPS, LANES), F32)], axis=0)
        path_rows = padded.T

        arrived(s_k, r_k, k_send, k_recv)
        new_keys = r_k[0]
        for i in range(1, NKV):
            new_keys = new_keys + r_k[i]
        new_keys = (inverse * new_keys).astype(BF16)
        q = by_head(g_q[mine].astype(F32) * (HEAD_DIM**-0.5), wide).astype(BF16)
        scores = nt_dot(q, new_keys)
        parts = []
        for h in range(HEADS):
            part = scores[h * PROPS : (h + 1) * PROPS] - path_rows[h : h + 1, :PROPS]
            parts.append(jnp.where(ancestry > 0.5, part, NEG))
        scores = jnp.concatenate(parts, axis=0)
        tree_top = jnp.max(scores, axis=1, keepdims=True)
        weights = jnp.exp(scores - tree_top)
        tree_total = jnp.sum(weights, axis=1, keepdims=True)
        arrived(s_v, r_v, v_send, v_recv)
        new_values = r_v[0].astype(F32)
        for i in range(1, NKV):
            new_values = new_values + r_v[i].astype(F32)
        new_values = (inverse * new_values).astype(BF16)
        tree_mix = diagonal(
            jnp.dot(weights.astype(BF16), new_values, preferred_element_type=F32), lane
        )
        tree_stats = jnp.zeros((PROPS, LANES), F32)
        for h in range(HEADS):
            rows = slice(h * PROPS, (h + 1) * PROPS)
            tree_stats = jnp.where(lane == h, tree_top[rows], tree_stats)
            tree_stats = jnp.where(lane == 3 * HEADS + h, tree_total[rows], tree_stats)

        arrived(s_mix, r_mix, m_send, m_recv)

        def stats_of(i):
            packed = r_mix[i, :, COLS:].astype(F32)
            one = pltpu.roll(packed, LANES - HEADS, 1)
            two = pltpu.roll(packed, LANES - 2 * HEADS, 1)
            return packed + (one + two)

        stats = [stats_of(i) for i in range(NKV)] + [tree_stats]
        best = functools.reduce(jnp.maximum, stats)
        factors = [jnp.exp(s - best) for s in stats]
        denominator = functools.reduce(
            jnp.add,
            [pltpu.roll(s, LANES - 3 * HEADS, 1) * f for s, f in zip(stats, factors)],
        )
        numerator = jnp.zeros((PROPS, COLS), F32)
        for i in range(NKV + 1):
            values = r_mix[i, :, :COLS].astype(F32) if i < NKV else tree_mix
            numerator = numerator + values * spread(
                [factors[i][:, h : h + 1] for h in range(HEADS)], lane
            )
        below = spread([denominator[:, h : h + 1] for h in range(HEADS)], lane)
        g_att[mine] = (numerator / below).astype(BF16)
        to_all(g_att, a_send, a_recv)

    pending.append(lambda: pl.when(is_owner)(lambda: sent_to_all(g_att, a_send, a_recv)))
    l_wo.wait()

    def await_attended(seq, carry):
        await_seq(g_att, a_send, a_recv, seq)
        return carry

    lax.fori_loop(0, SEQS, await_attended, 0)
    attended = jnp.concatenate([g_att[s].astype(F32) for s in range(SEQS)], axis=0).astype(BF16)
    f_term[...] = jnp.dot(attended, v_wo[...], preferred_element_type=F32)

    def term_copy(to, source):
        return pltpu.make_async_remote_copy(
            src_ref=s_term.at[to],
            dst_ref=out_ref.at[source],
            send_sem=t_send.at[to],
            recv_sem=t_recv.at[source],
            device_id={"tp": to},
            device_id_type=MESH,
        )

    for t in range(NTP):
        s_term[t] = f_term[t * OUT_ROWS : (t + 1) * OUT_ROWS, :].astype(BF16)

    def send_term(r, carry):
        term_copy(lax.rem(tp + r, NTP), tp).start()
        return carry

    lax.fori_loop(1, NTP, send_term, 0)
    out_ref[tp] = s_term[tp]

    def term_arrived(r, carry):
        source = lax.rem(tp + r, NTP)
        term_copy(source, source).wait_recv()
        return carry

    lax.fori_loop(1, NTP, term_arrived, 0)

    def term_sent(r, carry):
        term_copy(lax.rem(tp + r, NTP), tp).wait_send()
        return carry

    lax.fori_loop(1, NTP, term_sent, 0)
    for wait in pending:
        wait()


def body(
    tokens,
    norm_gain,
    query_weight,
    key_weight,
    value_weight,
    gate_weight,
    gate_bias,
    out_weight,
    cache_keys,
    cache_values,
    cache_decay,
    lengths,
    parents,
):
    anywhere = pl.BlockSpec(memory_space=pl.ANY)
    scalars = pl.BlockSpec(memory_space=pltpu.SMEM)
    vector = pl.BlockSpec(memory_space=pltpu.VMEM)
    dma = pltpu.SemaphoreType.DMA
    terms = pl.pallas_call(
        kernel,
        out_shape=jax.ShapeDtypeStruct((NTP, OUT_ROWS, COLS), BF16),
        in_specs=[anywhere] * 6 + [scalars] + [anywhere] * 4 + [scalars, vector],
        out_specs=vector,
        scratch_shapes=[
            pltpu.VMEM((ROWS, COLS), BF16),
            pltpu.VMEM((1, COLS), F32),
            pltpu.VMEM((COLS, COLS), BF16),
            pltpu.VMEM((COLS, COLS), BF16),
            pltpu.VMEM((COLS, COLS), BF16),
            pltpu.VMEM((32, COLS), BF16),
            pltpu.VMEM((COLS, COLS), BF16),
            pltpu.VMEM((SEQS, POS, COLS), BF16),
            pltpu.VMEM((SEQS, POS, COLS), BF16),
            pltpu.VMEM((SEQS, HEADS, POS), F32),
            pltpu.VMEM((SEQS, PROPS, COLS + LANES), F32),
            pltpu.VMEM((SEQS, PROPS, COLS), F32),
            pltpu.VMEM((SEQS, PROPS, COLS), BF16),
            pltpu.VMEM((NKV, PROPS, COLS + LANES), F32),
            pltpu.VMEM((NKV, PROPS, COLS), F32),
            pltpu.VMEM((NKV, PROPS, COLS), BF16),
            pltpu.VMEM((SEQS, PROPS, COLS), BF16),
            pltpu.VMEM((SEQS, PROPS, COLS + LANES), BF16),
            pltpu.VMEM((NKV, PROPS, COLS + LANES), BF16),
            pltpu.VMEM((SEQS, PROPS, COLS), BF16),
            pltpu.VMEM((ROWS, COLS), F32),
            pltpu.VMEM((NTP, OUT_ROWS, COLS), BF16),
            dma((10,)),
            dma((SEQS,)),
            dma((NKV,)),
            dma((SEQS,)),
            dma((NKV,)),
            dma((SEQS,)),
            dma((NKV,)),
            dma((NKV,)),
            dma((SEQS,)),
            dma((SEQS,)),
            dma((NKV,)),
            dma((NKV,)),
            dma((SEQS,)),
            dma((NTP,)),
            dma((NTP,)),
        ],
        compiler_params=pltpu.CompilerParams(
            collective_id=0, has_side_effects=True, vmem_limit_bytes=60 * 1024 * 1024
        ),
        name="tree_attention",
    )(
        tokens,
        norm_gain.reshape(1, -1),
        query_weight,
        key_weight,
        value_weight,
        gate_weight.T,
        gate_bias,
        out_weight,
        cache_keys,
        cache_values,
        cache_decay,
        lengths,
        parents,
    )
    return jnp.sum(terms.astype(F32), axis=0).astype(BF16)


def solution(mesh):
    in_specs = (
        P(None, "kv"),
        P("kv"),
        P("kv", "tp"),
        P("kv", "tp"),
        P("kv", "tp"),
        P(),
        P(),
        P("tp", "kv"),
        P(None, "kv", "tp"),
        P(None, "kv", "tp"),
        P(None, "tp", "kv"),
        P(),
        P(),
    )
    out_specs = P("tp", "kv")
    return jax.shard_map(body, mesh=mesh, in_specs=in_specs, out_specs=out_specs, check_vma=False)
```

```python
import functools

import jax
import jax.numpy as jnp
from jax import lax
from jax.experimental import pallas as pl
from jax.experimental.pallas import tpu as pltpu
from jax.sharding import PartitionSpec as P

MESH = pl.DeviceIdType.MESH
F32 = jnp.float32
BF16 = jnp.bfloat16
NKV = 16
NTP = 8
SEQS = 12
PROPS = 24
POS = 384
HEADS = 4
HEAD_DIM = 64
COLS = HEADS * HEAD_DIM
ROWS = SEQS * PROPS
OUT_ROWS = ROWS // NTP
LANES = 128
FULL_WIDTH = 4096.0
NEG = -1e30
GROUP = 3
HALF = 16


def nt_dot(a, b, precision=None):
    return lax.dot_general(
        a, b, (((1,), (1,)), ((), ())), preferred_element_type=F32, precision=precision
    )


def below(value, count):
    return jnp.where(value >= count, value - count, value)


def third(value):
    part = (
        jnp.where(value >= 3, 1, 0) + jnp.where(value >= 6, 1, 0) + jnp.where(value >= 9, 1, 0)
    )
    return part, value - 3 * part


def owner_of(seq):
    group, place = third(seq)
    row = below(group + 4 - place, 4)
    return 4 * row + place + jnp.where(place >= row, 1, 0)


def seq_at(index):
    row, place = third(index)
    return 3 * below(row + place, 4) + place


def spread(columns, lane):
    halves = []
    for pair in range(2):
        halves.append(jnp.where(lane < HEAD_DIM, columns[2 * pair], columns[2 * pair + 1]))
    return jnp.concatenate(halves, axis=1)


def diagonal(stacked, lane):
    halves = []
    for pair in range(2):
        even = stacked[(2 * pair) * PROPS : (2 * pair + 1) * PROPS, pair * LANES : (pair + 1) * LANES]
        odd = stacked[
            (2 * pair + 1) * PROPS : (2 * pair + 2) * PROPS, pair * LANES : (pair + 1) * LANES
        ]
        halves.append(jnp.where(lane < HEAD_DIM, even, odd))
    return jnp.concatenate(halves, axis=1)


def by_head(q, wide):
    parts = [
        jnp.where((wide >= h * HEAD_DIM) & (wide < (h + 1) * HEAD_DIM), q, 0.0)
        for h in range(HEADS)
    ]
    return jnp.concatenate(parts, axis=0)


def in_three(x):
    high = x.astype(BF16).astype(F32)
    rest = x - high
    mid = rest.astype(BF16).astype(F32)
    return high, mid, rest - mid


def kernel(
    tokens,
    gain,
    wq,
    wk,
    wv,
    gw,
    bias,
    wo,
    ckeys,
    cvals,
    cdecay,
    lengths,
    parents,
    out_ref,
    v_tok,
    v_gain,
    v_wq,
    v_wk,
    v_wv,
    v_gw,
    v_wo,
    v_ck,
    v_cv,
    v_cd,
    v_len,
    v_bias,
    v_par,
    s_q,
    s_k,
    s_v,
    r_q,
    r_k,
    r_v,
    g_q,
    s_mix,
    r_mix,
    s_att,
    s_half,
    r_att,
    r_half,
    load_sem,
    q_send,
    q_recv,
    k_send,
    k_recv,
    v_send,
    v_recv,
    gq_send,
    gq_recv,
    m_send,
    m_recv,
    a_send,
    a_recv,
    w_send,
    w_recv,
):
    kv = lax.axis_index("kv")
    tp = lax.axis_index("tp")
    row, column = lax.div(kv, 4), lax.rem(kv, 4)
    is_owner = row != column
    index = 3 * row + jnp.minimum(jnp.where(column > row, column - 1, column), 2)
    mine = seq_at(index)
    out_group, out_place = third(mine)
    whole_to = 2 * out_group + jnp.where(out_place == 2, 1, 0)
    is_whole = is_owner & (out_place != 1)
    is_half = is_owner & (out_place == 1)
    out_third = lax.div(tp, 2)
    odd = tp - 2 * out_third
    sources = [owner_of(3 * out_third + 2 * odd), owner_of(3 * out_third + 1)]

    gate_cols = gw.at[:, pl.ds(pl.multiple_of(kv * COLS, COLS), COLS)]
    loads = [
        pltpu.make_async_copy(src, dst, load_sem.at[n])
        for n, (src, dst) in enumerate(
            [
                (tokens, v_tok),
                (gain, v_gain),
                (wq, v_wq),
                (gate_cols, v_gw),
                (wk, v_wk),
                (wv, v_wv),
                (ckeys, v_ck),
                (cdecay, v_cd),
                (cvals, v_cv),
                (wo, v_wo.at[tp]),
                (lengths, v_len),
                (bias, v_bias),
                (parents, v_par),
            ]
        )
    ]
    for load in loads:
        load.start()
    l_tok, l_gain, l_wq, l_gw, l_wk, l_wv, l_ck, l_cd, l_cv, l_wo, l_len, l_bias, l_par = loads

    barrier = pltpu.get_barrier_semaphore()
    for r in range(1, NKV):
        pl.semaphore_signal(
            barrier, inc=1, device_id={"kv": below(kv + r, NKV)}, device_id_type=MESH
        )
    for r in range(1, NTP):
        pl.semaphore_signal(
            barrier, inc=1, device_id={"tp": below(tp + r, NTP)}, device_id_type=MESH
        )
    greeted = NKV - 1 + NTP - 1
    greeted = greeted + jnp.where(is_whole, NKV, 0) + jnp.where(is_half, 2 * NKV, 0)
    greeted = greeted - jnp.where(is_whole & (tp == whole_to), 1, 0)
    greeted = greeted - jnp.where(is_half & (out_third == out_group), 1, 0)
    for source in sources:
        for group in range(NTP):

            @pl.when((source != kv) | (tp != group))
            def _():
                pl.semaphore_signal(
                    barrier, inc=1, device_id={"kv": source, "tp": group}, device_id_type=MESH
                )

    lane = lax.broadcasted_iota(jnp.int32, (PROPS, LANES), 1)
    wide = lax.broadcasted_iota(jnp.int32, (PROPS, COLS), 1)

    def exchange(src, dst, send, recv, seq):
        return pltpu.make_async_remote_copy(
            src_ref=src.at[seq],
            dst_ref=dst.at[kv],
            send_sem=send.at[seq],
            recv_sem=recv.at[kv],
            device_id={"kv": owner_of(seq)},
            device_id_type=MESH,
        )

    def to_owners(src, dst, send, recv):
        def step(j, carry):
            seq = seq_at(below(index + j, SEQS))

            @pl.when(owner_of(seq) != kv)
            def _():
                exchange(src, dst, send, recv, seq).start()

            return carry

        lax.fori_loop(0, SEQS, step, 0)

    def sent_to_owners(src, dst, send, recv):
        for seq in range(SEQS):

            @pl.when(owner_of(seq) != kv)
            def _():
                exchange(src, dst, send, recv, seq).wait_send()

    def arrived(src, dst, send, recv):
        def step(i, carry):
            @pl.when(i != kv)
            def _():
                pltpu.make_async_remote_copy(
                    src_ref=src.at[0],
                    dst_ref=dst.at[i],
                    send_sem=send.at[0],
                    recv_sem=recv.at[i],
                    device_id={"kv": i},
                    device_id_type=MESH,
                ).wait_recv()

            return carry

        lax.fori_loop(0, NKV, step, 0)

    def gather_copy(buf, send, recv, peer, slot, seq):
        return pltpu.make_async_remote_copy(
            src_ref=buf.at[seq],
            dst_ref=buf.at[seq],
            send_sem=send.at[slot],
            recv_sem=recv.at[seq],
            device_id={"kv": peer},
            device_id_type=MESH,
        )

    def to_all(buf, send, recv):
        def step(r, carry):
            gather_copy(buf, send, recv, below(kv + r, NKV), r, mine).start()
            return carry

        lax.fori_loop(1, NKV, step, 0)

    def sent_to_all(buf, send, recv):
        for r in range(1, NKV):
            gather_copy(buf, send, recv, below(kv + r, NKV), r, mine).wait_send()

    def whole_copy(r):
        return pltpu.make_async_remote_copy(
            src_ref=s_att,
            dst_ref=r_att.at[tp],
            send_sem=a_send.at[r],
            recv_sem=a_recv.at[tp],
            device_id={"kv": below(kv + r, NKV), "tp": whole_to},
            device_id_type=MESH,
        )

    def half_copy(r, c):
        return pltpu.make_async_remote_copy(
            src_ref=s_half.at[c],
            dst_ref=r_half.at[tp],
            send_sem=a_send.at[NKV * c + r],
            recv_sem=a_recv.at[NTP + tp],
            device_id={"kv": below(kv + r, NKV), "tp": 2 * out_group + c},
            device_id_type=MESH,
        )

    def await_seq(buf, send, recv, seq):
        @pl.when(owner_of(seq) != kv)
        def _():
            gather_copy(buf, send, recv, owner_of(seq), 0, seq).wait_recv()

    pending = []

    l_tok.wait()
    l_gain.wait()
    x = v_tok[...].astype(F32)
    squares = jnp.sum(x * x, axis=1, keepdims=True)
    normed = (x * v_gain[...]).astype(BF16)
    l_wq.wait()
    s_q[:, :, 0:COLS] = jnp.dot(normed, v_wq[...], preferred_element_type=F32).reshape(
        SEQS, PROPS, COLS
    )
    l_gw.wait()
    pick_row = lax.broadcasted_iota(jnp.int32, (LANES, 32), 0)
    pick_col = lax.broadcasted_iota(jnp.int32, (LANES, 32), 1)
    pick = (pick_col == tp * HEADS + pick_row) & (pick_row < HEADS)
    own_gates = jnp.dot(
        pick.astype(F32).astype(BF16), v_gw[...], preferred_element_type=F32
    ).astype(BF16)
    extra = nt_dot(normed, own_gates)
    lane_rows = lax.broadcasted_iota(jnp.int32, (ROWS, LANES), 1)
    extra = jnp.where(lane_rows < HEADS, extra, squares)
    s_q[:, :, COLS:] = extra.reshape(SEQS, PROPS, LANES)

    pl.semaphore_wait(barrier, greeted)
    to_owners(s_q, r_q, q_send, q_recv)
    pending.append(lambda: sent_to_owners(s_q, r_q, q_send, q_recv))

    def weight_copy(to, source):
        return pltpu.make_async_remote_copy(
            src_ref=v_wo.at[source],
            dst_ref=v_wo.at[source],
            send_sem=w_send.at[to],
            recv_sem=w_recv.at[source],
            device_id={"tp": to},
            device_id_type=MESH,
        )

    def send_weight(r, carry):
        weight_copy(below(tp + r, NTP), tp).start()
        return carry

    def weight_sent(r, carry):
        weight_copy(below(tp + r, NTP), tp).wait_send()
        return carry

    def weight_arrived(r, carry):
        source = below(tp + r, NTP)
        weight_copy(source, source).wait_recv()
        return carry

    l_wo.wait()
    lax.fori_loop(1, NTP, send_weight, 0)
    pending.append(lambda: lax.fori_loop(1, NTP, weight_sent, 0))

    l_wk.wait()
    s_k[...] = jnp.dot(normed, v_wk[...], preferred_element_type=F32).reshape(SEQS, PROPS, COLS)
    l_wv.wait()
    new = jnp.dot(normed, v_wv[...], preferred_element_type=F32)
    s_v[...] = new.astype(BF16).reshape(SEQS, PROPS, COLS)

    @pl.when(is_owner)
    def _():
        r_q[kv] = s_q[mine]
        arrived(s_q, r_q, q_send, q_recv)
        total = r_q[0]
        for i in range(1, NKV):
            total = total + r_q[i]
        s_q[mine] = total
        inverse = lax.rsqrt(total[:, COLS + HEADS : COLS + HEADS + 1] / FULL_WIDTH + 1e-6)
        g_q[mine] = (inverse * total[:, :COLS]).astype(BF16)
        to_all(g_q, gq_send, gq_recv)

    pending.append(lambda: pl.when(is_owner)(lambda: sent_to_all(g_q, gq_send, gq_recv)))
    to_owners(s_k, r_k, k_send, k_recv)
    pending.append(lambda: sent_to_owners(s_k, r_k, k_send, k_recv))
    to_owners(s_v, r_v, v_send, v_recv)
    pending.append(lambda: sent_to_owners(s_v, r_v, v_send, v_recv))

    l_ck.wait()
    l_cd.wait()
    l_len.wait()
    l_bias.wait()
    l_par.wait()
    l_cv.wait()
    position = kv * POS + lax.broadcasted_iota(jnp.int32, (1, POS), 1)

    def attend(seq):
        q = by_head(g_q[seq].astype(F32) * (HEAD_DIM**-0.5), wide).astype(BF16)
        scores = nt_dot(q, v_ck[seq])
        live = position < v_len[seq]
        parts = []
        for h in range(HEADS):
            decay = jnp.where(live, v_cd[seq, h : h + 1, :], NEG)
            parts.append(scores[h * PROPS : (h + 1) * PROPS] + decay)
        scores = jnp.concatenate(parts, axis=0)
        top = jnp.max(scores, axis=1, keepdims=True)
        weights = jnp.exp(scores - top)
        total = jnp.sum(weights, axis=1, keepdims=True)
        mix = jnp.dot(weights.astype(BF16), v_cv[seq], preferred_element_type=F32)
        stats = jnp.zeros((PROPS, LANES), F32)
        for h in range(HEADS):
            rows = slice(h * PROPS, (h + 1) * PROPS)
            for n, piece in enumerate(in_three(top[rows]) + in_three(total[rows])):
                stats = jnp.where(lane == n * HEADS + h, piece, stats)
        s_mix[seq] = jnp.concatenate([diagonal(mix, lane), stats], axis=1).astype(BF16)

    def attend_group(j, carry):
        seqs = [seq_at(below(index + SEQS - j * GROUP - u, SEQS)) for u in range(GROUP)]
        for seq in seqs:
            await_seq(g_q, gq_send, gq_recv, seq)
        for seq in seqs:
            attend(seq)
        for seq in seqs:

            @pl.when(owner_of(seq) != kv)
            def _():
                exchange(s_mix, r_mix, m_send, m_recv, seq).start()

        return carry

    lax.fori_loop(0, SEQS // GROUP, attend_group, 0)

    pending.append(lambda: sent_to_owners(s_mix, r_mix, m_send, m_recv))
    @pl.when(is_owner)
    def _():
        r_k[kv] = s_k[mine]
        r_v[kv] = s_v[mine]
        r_mix[kv] = s_mix[mine]
        summed = s_q[mine]
        inverse = lax.rsqrt(summed[:, COLS + HEADS : COLS + HEADS + 1] / FULL_WIDTH + 1e-6)
        gates = inverse * summed[:, COLS:]
        shift = jnp.zeros((PROPS, LANES), F32)
        for h in range(HEADS):
            shift = jnp.where(lane == h, v_bias[tp * HEADS + h], shift)
        gates = gates + shift
        log_gates = jnp.minimum(gates, 0.0) - jnp.log1p(jnp.exp(-jnp.abs(gates)))
        square = (PROPS, PROPS)
        older = lax.broadcasted_iota(jnp.int32, square, 0)
        younger = lax.broadcasted_iota(jnp.int32, square, 1)
        linked = (older == v_par[pl.ds(mine, 1), :]) | (older == younger)
        up = linked.astype(F32)
        for _ in range(5):
            closed = up.astype(BF16)
            up = jnp.minimum(jnp.dot(closed, closed, preferred_element_type=F32), 1.0)
        eye = (older == younger).astype(F32)
        ancestry = nt_dot(eye.astype(BF16), up.astype(BF16))
        path = jnp.dot(
            ancestry, log_gates, preferred_element_type=F32, precision=lax.Precision.HIGHEST
        )
        padded = jnp.concatenate([path, jnp.zeros((LANES - PROPS, LANES), F32)], axis=0)
        path_rows = padded.T

        arrived(s_k, r_k, k_send, k_recv)
        new_keys = r_k[0]
        for i in range(1, NKV):
            new_keys = new_keys + r_k[i]
        new_keys = (inverse * new_keys).astype(BF16)
        q = by_head(g_q[mine].astype(F32) * (HEAD_DIM**-0.5), wide).astype(BF16)
        scores = nt_dot(q, new_keys)
        parts = []
        for h in range(HEADS):
            part = scores[h * PROPS : (h + 1) * PROPS] - path_rows[h : h + 1, :PROPS]
            parts.append(jnp.where(ancestry > 0.5, part, NEG))
        scores = jnp.concatenate(parts, axis=0)
        tree_top = jnp.max(scores, axis=1, keepdims=True)
        weights = jnp.exp(scores - tree_top)
        tree_total = jnp.sum(weights, axis=1, keepdims=True)
        arrived(s_v, r_v, v_send, v_recv)
        new_values = r_v[0].astype(F32)
        for i in range(1, NKV):
            new_values = new_values + r_v[i].astype(F32)
        new_values = (inverse * new_values).astype(BF16)
        tree_mix = diagonal(
            jnp.dot(weights.astype(BF16), new_values, preferred_element_type=F32), lane
        )
        tree_stats = jnp.zeros((PROPS, LANES), F32)
        for h in range(HEADS):
            rows = slice(h * PROPS, (h + 1) * PROPS)
            tree_stats = jnp.where(lane == h, tree_top[rows], tree_stats)
            tree_stats = jnp.where(lane == 3 * HEADS + h, tree_total[rows], tree_stats)

        arrived(s_mix, r_mix, m_send, m_recv)

        def stats_of(i):
            packed = r_mix[i, :, COLS:].astype(F32)
            one = pltpu.roll(packed, LANES - HEADS, 1)
            two = pltpu.roll(packed, LANES - 2 * HEADS, 1)
            return packed + (one + two)

        stats = [stats_of(i) for i in range(NKV)] + [tree_stats]
        best = functools.reduce(jnp.maximum, stats)
        factors = [jnp.exp(s - best) for s in stats]
        denominator = functools.reduce(
            jnp.add,
            [pltpu.roll(s, LANES - 3 * HEADS, 1) * f for s, f in zip(stats, factors)],
        )
        numerator = jnp.zeros((PROPS, COLS), F32)
        for i in range(NKV + 1):
            values = r_mix[i, :, :COLS].astype(F32) if i < NKV else tree_mix
            numerator = numerator + values * spread(
                [factors[i][:, h : h + 1] for h in range(HEADS)], lane
            )
        under = spread([denominator[:, h : h + 1] for h in range(HEADS)], lane)
        attended = numerator / under

        @pl.when(out_place != 1)
        def _():
            s_att[...] = attended.astype(BF16)

            def step(r, carry):
                whole_copy(r).start()
                return carry

            lax.fori_loop(1, NKV, step, 0)

            @pl.when(tp != whole_to)
            def _():
                whole_copy(0).start()

            @pl.when(tp == whole_to)
            def _():
                r_att[tp] = s_att[...]

        @pl.when(out_place == 1)
        def _():
            s_half[0] = attended[:HALF].astype(BF16)
            s_half[1] = attended[PROPS - HALF :].astype(BF16)

            def step(r, carry):
                half_copy(r, 0).start()
                half_copy(r, 1).start()
                return carry

            lax.fori_loop(1, NKV, step, 0)
            for c in range(2):

                @pl.when(tp != 2 * out_group + c)
                def _():
                    half_copy(0, c).start()

                @pl.when(tp == 2 * out_group + c)
                def _():
                    r_half[tp] = s_half[c]

    def scattered():
        @pl.when(is_whole)
        def _():
            for r in range(1, NKV):
                whole_copy(r).wait_send()

            @pl.when(tp != whole_to)
            def _():
                whole_copy(0).wait_send()

        @pl.when(is_half)
        def _():
            for c in range(2):
                for r in range(1, NKV):
                    half_copy(r, c).wait_send()

                @pl.when(tp != 2 * out_group + c)
                def _():
                    half_copy(0, c).wait_send()

    lax.fori_loop(1, NTP, weight_arrived, 0)
    for wait in pending:
        wait()

    for group in range(NTP):

        @pl.when((sources[0] != kv) | (tp != group))
        def _():
            pltpu.make_async_remote_copy(
                src_ref=s_att,
                dst_ref=r_att.at[group],
                send_sem=a_send.at[0],
                recv_sem=a_recv.at[group],
                device_id={"kv": sources[0], "tp": group},
                device_id_type=MESH,
            ).wait_recv()

        @pl.when((sources[1] != kv) | (tp != group))
        def _():
            pltpu.make_async_remote_copy(
                src_ref=s_half.at[0],
                dst_ref=r_half.at[group],
                send_sem=a_send.at[0],
                recv_sem=a_recv.at[NTP + group],
                device_id={"kv": sources[1], "tp": group},
                device_id_type=MESH,
            ).wait_recv()

    mixed = jnp.zeros((PROPS + HALF, COLS), F32)
    for group in range(NTP):
        whole, half = r_att[group].astype(F32), r_half[group].astype(F32)
        both = jnp.where(
            odd == 1,
            jnp.concatenate([half, whole], axis=0),
            jnp.concatenate([whole, half], axis=0),
        )
        term = jnp.dot(both.astype(BF16), v_wo[group], preferred_element_type=F32)
        mixed = mixed + term.astype(BF16).astype(F32)
    out_ref[...] = jnp.where(
        odd == 1, mixed[PROPS + HALF - OUT_ROWS :], mixed[:OUT_ROWS]
    ).astype(BF16)
    scattered()


def body(
    tokens,
    norm_gain,
    query_weight,
    key_weight,
    value_weight,
    gate_weight,
    gate_bias,
    out_weight,
    cache_keys,
    cache_values,
    cache_decay,
    lengths,
    parents,
):
    anywhere = pl.BlockSpec(memory_space=pl.ANY)
    vector = pl.BlockSpec(memory_space=pltpu.VMEM)
    dma = pltpu.SemaphoreType.DMA
    return pl.pallas_call(
        kernel,
        out_shape=jax.ShapeDtypeStruct((OUT_ROWS, COLS), BF16),
        in_specs=[anywhere] * 13,
        out_specs=vector,
        scratch_shapes=[
            pltpu.VMEM((ROWS, COLS), BF16),
            pltpu.VMEM((1, COLS), F32),
            pltpu.VMEM((COLS, COLS), BF16),
            pltpu.VMEM((COLS, COLS), BF16),
            pltpu.VMEM((COLS, COLS), BF16),
            pltpu.VMEM((32, COLS), BF16),
            pltpu.VMEM((NTP, COLS, COLS), BF16),
            pltpu.VMEM((SEQS, POS, COLS), BF16),
            pltpu.VMEM((SEQS, POS, COLS), BF16),
            pltpu.VMEM((SEQS, HEADS, POS), F32),
            pltpu.SMEM((SEQS,), jnp.int32),
            pltpu.SMEM((NTP * HEADS,), F32),
            pltpu.VMEM((SEQS, PROPS), jnp.int32),
            pltpu.VMEM((SEQS, PROPS, COLS + LANES), F32),
            pltpu.VMEM((SEQS, PROPS, COLS), F32),
            pltpu.VMEM((SEQS, PROPS, COLS), BF16),
            pltpu.VMEM((NKV, PROPS, COLS + LANES), F32),
            pltpu.VMEM((NKV, PROPS, COLS), F32),
            pltpu.VMEM((NKV, PROPS, COLS), BF16),
            pltpu.VMEM((SEQS, PROPS, COLS), BF16),
            pltpu.VMEM((SEQS, PROPS, COLS + LANES), BF16),
            pltpu.VMEM((NKV, PROPS, COLS + LANES), BF16),
            pltpu.VMEM((PROPS, COLS), BF16),
            pltpu.VMEM((2, HALF, COLS), BF16),
            pltpu.VMEM((NTP, PROPS, COLS), BF16),
            pltpu.VMEM((NTP, HALF, COLS), BF16),
            dma((13,)),
            dma((SEQS,)),
            dma((NKV,)),
            dma((SEQS,)),
            dma((NKV,)),
            dma((SEQS,)),
            dma((NKV,)),
            dma((NKV,)),
            dma((SEQS,)),
            dma((SEQS,)),
            dma((NKV,)),
            dma((2 * NKV,)),
            dma((2 * NTP,)),
            dma((NTP,)),
            dma((NTP,)),
        ],
        compiler_params=pltpu.CompilerParams(
            collective_id=0, has_side_effects=True, vmem_limit_bytes=60 * 1024 * 1024
        ),
        name="tree_attention",
    )(
        tokens,
        norm_gain.reshape(1, -1),
        query_weight,
        key_weight,
        value_weight,
        gate_weight.T,
        gate_bias,
        out_weight,
        cache_keys,
        cache_values,
        cache_decay,
        lengths,
        parents,
    )


def solution(mesh):
    in_specs = (
        P(None, "kv"),
        P("kv"),
        P("kv", "tp"),
        P("kv", "tp"),
        P("kv", "tp"),
        P(),
        P(),
        P("tp", "kv"),
        P(None, "kv", "tp"),
        P(None, "kv", "tp"),
        P(None, "tp", "kv"),
        P(),
        P(),
    )
    out_specs = P("tp", "kv")
    return jax.shard_map(body, mesh=mesh, in_specs=in_specs, out_specs=out_specs, check_vma=False)
```

```python
import functools

import jax
import jax.numpy as jnp
from jax import lax
from jax.experimental import pallas as pl
from jax.experimental.pallas import tpu as pltpu
from jax.sharding import PartitionSpec as P

MESH = pl.DeviceIdType.MESH
F32 = jnp.float32
BF16 = jnp.bfloat16
NKV = 16
NTP = 8
SEQS = 12
PROPS = 24
POS = 384
HEADS = 4
HEAD_DIM = 64
COLS = HEADS * HEAD_DIM
ROWS = SEQS * PROPS
OUT_ROWS = ROWS // NTP
LANES = 128
FULL_WIDTH = 4096.0
NEG = -1e30
GROUP = 3
HALF = 16
FEW = 8
FAR_FIRST = sorted(
    [(z, x) for z in range(4) for x in range(4) if z or x],
    key=lambda d: -sum(min(n, 4 - n) for n in d),
)


def nt_dot(a, b, precision=None):
    return lax.dot_general(
        a, b, (((1,), (1,)), ((), ())), preferred_element_type=F32, precision=precision
    )


def below(value, count):
    return jnp.where(value >= count, value - count, value)


def third(value):
    part = (
        jnp.where(value >= 3, 1, 0) + jnp.where(value >= 6, 1, 0) + jnp.where(value >= 9, 1, 0)
    )
    return part, value - 3 * part


def owner_of(seq):
    group, place = third(seq)
    row = below(group + 4 - place, 4)
    return 4 * row + place + jnp.where(place >= row, 1, 0)


def seq_at(index):
    row, place = third(index)
    return 3 * below(row + place, 4) + place


def spread(columns, lane):
    halves = []
    for pair in range(2):
        halves.append(jnp.where(lane < HEAD_DIM, columns[2 * pair], columns[2 * pair + 1]))
    return jnp.concatenate(halves, axis=1)


def diagonal(stacked, lane):
    halves = []
    for pair in range(2):
        even = stacked[(2 * pair) * PROPS : (2 * pair + 1) * PROPS, pair * LANES : (pair + 1) * LANES]
        odd = stacked[
            (2 * pair + 1) * PROPS : (2 * pair + 2) * PROPS, pair * LANES : (pair + 1) * LANES
        ]
        halves.append(jnp.where(lane < HEAD_DIM, even, odd))
    return jnp.concatenate(halves, axis=1)


def by_head(q, wide):
    parts = [
        jnp.where((wide >= h * HEAD_DIM) & (wide < (h + 1) * HEAD_DIM), q, 0.0)
        for h in range(HEADS)
    ]
    return jnp.concatenate(parts, axis=0)


def kernel(
    tokens,
    gain,
    wq,
    wk,
    wv,
    gw,
    bias,
    wo,
    ckeys,
    cvals,
    cdecay,
    lengths,
    parents,
    out_ref,
    v_tok,
    v_gain,
    v_wq,
    v_wk,
    v_wv,
    v_gw,
    v_wo,
    v_ck,
    v_cv,
    v_cd,
    v_len,
    v_bias,
    v_par,
    s_q,
    s_sq,
    s_x,
    s_k,
    s_v,
    r_q,
    r_sq,
    r_x,
    r_k,
    r_v,
    g_q,
    i_row,
    i_col,
    s_mix,
    s_stat,
    r_mix,
    r_stat,
    s_att,
    s_half,
    r_att,
    r_half,
    load_sem,
    q_send,
    q_recv,
    z_send,
    z_recv,
    x_send,
    x_recv,
    k_send,
    k_recv,
    v_send,
    v_recv,
    gq_send,
    gq_recv,
    m_send,
    m_recv,
    y_send,
    y_recv,
    a_send,
    a_recv,
    w_send,
    w_recv,
):
    kv = lax.axis_index("kv")
    tp = lax.axis_index("tp")
    row, column = lax.div(kv, 4), lax.rem(kv, 4)
    is_owner = row != column
    index = 3 * row + jnp.minimum(jnp.where(column > row, column - 1, column), 2)
    mine = seq_at(index)
    out_group, out_place = third(mine)
    whole_to = 2 * out_group + jnp.where(out_place == 2, 1, 0)
    is_whole = is_owner & (out_place != 1)
    is_half = is_owner & (out_place == 1)
    out_third = lax.div(tp, 2)
    odd = tp - 2 * out_third
    sources = [owner_of(3 * out_third + 2 * odd), owner_of(3 * out_third + 1)]

    gate_cols = gw.at[:, pl.ds(pl.multiple_of(kv * COLS, COLS), COLS)]
    loads = [
        pltpu.make_async_copy(src, dst, load_sem.at[n])
        for n, (src, dst) in enumerate(
            [
                (tokens, v_tok),
                (gain, v_gain),
                (wq, v_wq),
                (gate_cols, v_gw),
                (wk, v_wk),
                (wv, v_wv),
                (ckeys, v_ck),
                (cdecay, v_cd),
                (cvals, v_cv),
                (wo, v_wo.at[tp]),
                (lengths, v_len),
                (bias, v_bias),
                (parents, v_par),
            ]
        )
    ]
    for load in loads:
        load.start()
    l_tok, l_gain, l_wq, l_gw, l_wk, l_wv, l_ck, l_cd, l_cv, l_wo, l_len, l_bias, l_par = loads

    barrier = pltpu.get_barrier_semaphore()
    for r in range(1, NKV):
        pl.semaphore_signal(
            barrier, inc=1, device_id={"kv": below(kv + r, NKV)}, device_id_type=MESH
        )
    for r in range(1, NTP):
        pl.semaphore_signal(
            barrier, inc=1, device_id={"tp": below(tp + r, NTP)}, device_id_type=MESH
        )
    greeted = NKV - 1 + NTP - 1
    greeted = greeted + jnp.where(is_whole, NKV, 0) + jnp.where(is_half, 2 * NKV, 0)
    greeted = greeted - jnp.where(is_whole & (tp == whole_to), 1, 0)
    greeted = greeted - jnp.where(is_half & (out_third == out_group), 1, 0)
    for source in sources:
        for group in range(NTP):

            @pl.when((source != kv) | (tp != group))
            def _():
                pl.semaphore_signal(
                    barrier, inc=1, device_id={"kv": source, "tp": group}, device_id_type=MESH
                )

    lane = lax.broadcasted_iota(jnp.int32, (PROPS, LANES), 1)
    wide = lax.broadcasted_iota(jnp.int32, (PROPS, COLS), 1)

    def exchange(src, dst, send, recv, seq):
        return pltpu.make_async_remote_copy(
            src_ref=src.at[seq],
            dst_ref=dst.at[kv],
            send_sem=send.at[seq],
            recv_sem=recv.at[kv],
            device_id={"kv": owner_of(seq)},
            device_id_type=MESH,
        )

    def at_distance(z, x):
        return below(row + z, 4), below(column + x, 4)

    def to_owners(src, dst, send, recv):
        for distance in FAR_FIRST:
            z, x = at_distance(*distance)

            @pl.when(z != x)
            def _():
                seq = seq_at(3 * z + jnp.where(x > z, x - 1, x))
                exchange(src, dst, send, recv, seq).start()

    def sent_to_owners(src, dst, send, recv):
        for seq in range(SEQS):

            @pl.when(owner_of(seq) != kv)
            def _():
                exchange(src, dst, send, recv, seq).wait_send()

    def arrived(src, dst, send, recv):
        def step(i, carry):
            @pl.when(i != kv)
            def _():
                pltpu.make_async_remote_copy(
                    src_ref=src.at[0],
                    dst_ref=dst.at[i],
                    send_sem=send.at[0],
                    recv_sem=recv.at[i],
                    device_id={"kv": i},
                    device_id_type=MESH,
                ).wait_recv()

            return carry

        lax.fori_loop(0, NKV, step, 0)

    def gather_copy(buf, send, recv, peer, slot, seq):
        return pltpu.make_async_remote_copy(
            src_ref=buf.at[seq],
            dst_ref=buf.at[seq],
            send_sem=send.at[slot],
            recv_sem=recv.at[seq],
            device_id={"kv": peer},
            device_id_type=MESH,
        )

    def to_all(buf, send, recv):
        for r in range(1, NKV):
            gather_copy(buf, send, recv, below(kv + r, NKV), r, mine).start()

    def sent_to_all(buf, send, recv):
        for r in range(1, NKV):
            gather_copy(buf, send, recv, below(kv + r, NKV), r, mine).wait_send()

    def whole_copy(distance):
        z, x = at_distance(*distance)
        return pltpu.make_async_remote_copy(
            src_ref=s_att,
            dst_ref=r_att.at[tp],
            send_sem=a_send.at[4 * distance[0] + distance[1]],
            recv_sem=a_recv.at[tp],
            device_id={"kv": 4 * z + x, "tp": whole_to},
            device_id_type=MESH,
        )

    def half_copy(distance, c):
        z, x = at_distance(*distance)
        return pltpu.make_async_remote_copy(
            src_ref=s_half.at[c],
            dst_ref=r_half.at[tp],
            send_sem=a_send.at[NKV * c + 4 * distance[0] + distance[1]],
            recv_sem=a_recv.at[NTP + tp],
            device_id={"kv": 4 * z + x, "tp": 2 * out_group + c},
            device_id_type=MESH,
        )

    def await_seq(buf, send, recv, seq):
        @pl.when(owner_of(seq) != kv)
        def _():
            gather_copy(buf, send, recv, owner_of(seq), 0, seq).wait_recv()

    pending = []

    l_tok.wait()
    l_gain.wait()
    x = v_tok[...].astype(F32)
    normed = (x * v_gain[...]).astype(BF16)
    l_wq.wait()
    s_q[...] = jnp.dot(normed, v_wq[...], preferred_element_type=F32).reshape(SEQS, PROPS, COLS)
    squares = x * x
    high = squares.astype(BF16)
    low = (squares - high.astype(F32)).astype(BF16)
    ones = jnp.ones((16, COLS), BF16)
    square_rows = nt_dot(ones, high) + nt_dot(ones, low)
    l_gw.wait()
    pick_row = lax.broadcasted_iota(jnp.int32, (16, 32), 0)
    pick_col = lax.broadcasted_iota(jnp.int32, (16, 32), 1)
    pick = (pick_col == tp * HEADS + pick_row) & (pick_row < HEADS)
    own_gates = jnp.dot(
        pick.astype(F32).astype(BF16), v_gw[...], preferred_element_type=F32
    ).astype(BF16)
    rows = jnp.where(
        lax.broadcasted_iota(jnp.int32, (FEW, ROWS), 0) < HEADS,
        nt_dot(own_gates, normed)[:FEW],
        square_rows[:FEW],
    )
    rows = jnp.concatenate([rows, jnp.zeros((FEW, 3 * LANES - ROWS), F32)], axis=1)
    for seq in range(SEQS):
        shift = (3 * LANES - seq * PROPS) % (3 * LANES)
        turned = pltpu.roll(rows, shift, 1) if shift else rows
        s_x[seq] = turned[:, :LANES]
        s_sq[seq] = turned[HEADS : HEADS + 1, :LANES]

    pl.semaphore_wait(barrier, greeted)
    to_owners(s_sq, r_sq, z_send, z_recv)
    to_owners(s_q, r_q, q_send, q_recv)
    pending.append(lambda: sent_to_owners(s_sq, r_sq, z_send, z_recv))
    pending.append(lambda: sent_to_owners(s_q, r_q, q_send, q_recv))

    def weight_copy(to, source):
        return pltpu.make_async_remote_copy(
            src_ref=v_wo.at[source],
            dst_ref=v_wo.at[source],
            send_sem=w_send.at[to],
            recv_sem=w_recv.at[source],
            device_id={"tp": to},
            device_id_type=MESH,
        )

    def send_weight(r, carry):
        weight_copy(below(tp + r, NTP), tp).start()
        return carry

    def weight_sent(r, carry):
        weight_copy(below(tp + r, NTP), tp).wait_send()
        return carry

    def weight_arrived(r, carry):
        source = below(tp + r, NTP)
        weight_copy(source, source).wait_recv()
        return carry

    l_wo.wait()
    lax.fori_loop(1, NTP, send_weight, 0)
    pending.append(lambda: lax.fori_loop(1, NTP, weight_sent, 0))

    l_wk.wait()
    s_k[...] = jnp.dot(normed, v_wk[...], preferred_element_type=F32).reshape(SEQS, PROPS, COLS)
    l_wv.wait()
    new = jnp.dot(normed, v_wv[...], preferred_element_type=F32)
    s_v[...] = new.astype(BF16).reshape(SEQS, PROPS, COLS)

    @pl.when(is_owner)
    def _():
        r_q[kv] = s_q[mine]
        r_sq[kv] = s_sq[mine]
        arrived(s_sq, r_sq, z_send, z_recv)
        summed = r_sq[0]
        for i in range(1, NKV):
            summed = summed + r_sq[i]
        i_row[...] = lax.rsqrt(summed / FULL_WIDTH + 1e-6)
        on_diagonal = lane == lax.broadcasted_iota(jnp.int32, (PROPS, LANES), 0)
        inverse = jnp.sum(jnp.where(on_diagonal, i_row[...], 0.0), axis=1, keepdims=True)
        i_col[...] = jnp.broadcast_to(inverse, (PROPS, LANES))
        arrived(s_q, r_q, q_send, q_recv)
        total = r_q[0]
        for i in range(1, NKV):
            total = total + r_q[i]
        g_q[mine] = (inverse * total).astype(BF16)
        to_all(g_q, gq_send, gq_recv)

    pending.append(lambda: pl.when(is_owner)(lambda: sent_to_all(g_q, gq_send, gq_recv)))
    to_owners(s_x, r_x, x_send, x_recv)
    pending.append(lambda: sent_to_owners(s_x, r_x, x_send, x_recv))
    to_owners(s_k, r_k, k_send, k_recv)
    pending.append(lambda: sent_to_owners(s_k, r_k, k_send, k_recv))
    to_owners(s_v, r_v, v_send, v_recv)
    pending.append(lambda: sent_to_owners(s_v, r_v, v_send, v_recv))

    l_ck.wait()
    l_cd.wait()
    l_len.wait()
    l_bias.wait()
    l_par.wait()
    l_cv.wait()
    position = kv * POS + lax.broadcasted_iota(jnp.int32, (1, POS), 1)

    def stat_rows(top, total):
        stats = jnp.zeros((PROPS, LANES), F32)
        for h in range(HEADS):
            own = slice(h * PROPS, (h + 1) * PROPS)
            stats = jnp.where(lane == h, top[own], stats)
            stats = jnp.where(lane == HEADS + h, total[own], stats)
        padded = jnp.concatenate([stats, jnp.zeros((LANES - PROPS, LANES), F32)], axis=0)
        return padded.T[:FEW]

    def attend(seq):
        q = by_head(g_q[seq].astype(F32) * (HEAD_DIM**-0.5), wide).astype(BF16)
        scores = nt_dot(q, v_ck[seq])
        live = position < v_len[seq]
        parts = []
        for h in range(HEADS):
            decay = jnp.where(live, v_cd[seq, h : h + 1, :], NEG)
            parts.append(scores[h * PROPS : (h + 1) * PROPS] + decay)
        scores = jnp.concatenate(parts, axis=0)
        top = jnp.max(scores, axis=1, keepdims=True)
        weights = jnp.exp(scores - top)
        total = jnp.sum(weights, axis=1, keepdims=True)
        mix = jnp.dot(weights.astype(BF16), v_cv[seq], preferred_element_type=F32)
        s_mix[seq] = diagonal(mix, lane).astype(BF16)
        s_stat[seq] = stat_rows(top, total)

    def attend_group(j, carry):
        seqs = [seq_at(below(index + SEQS - j * GROUP - u, SEQS)) for u in range(GROUP)]
        for seq in seqs:
            await_seq(g_q, gq_send, gq_recv, seq)
        for seq in seqs:
            attend(seq)
        for seq in seqs:

            @pl.when(owner_of(seq) != kv)
            def _():
                exchange(s_stat, r_stat, y_send, y_recv, seq).start()
                exchange(s_mix, r_mix, m_send, m_recv, seq).start()

        return carry

    lax.fori_loop(0, SEQS // GROUP, attend_group, 0)

    pending.append(lambda: sent_to_owners(s_mix, r_mix, m_send, m_recv))
    pending.append(lambda: sent_to_owners(s_stat, r_stat, y_send, y_recv))
    @pl.when(is_owner)
    def _():
        r_k[kv] = s_k[mine]
        r_v[kv] = s_v[mine]
        r_mix[kv] = s_mix[mine]
        r_stat[kv] = s_stat[mine]
        r_x[kv] = s_x[mine]
        inverse = i_col[:, 0:1]
        head_row = lax.broadcasted_iota(jnp.int32, (FEW, LANES), 0)
        shift = jnp.zeros((FEW, LANES), F32)
        for h in range(HEADS):
            shift = jnp.where(head_row == h, v_bias[tp * HEADS + h], shift)
        arrived(s_x, r_x, x_send, x_recv)
        gates = r_x[0]
        for i in range(1, NKV):
            gates = gates + r_x[i]
        gates = i_row[...] * gates + shift
        log_gates = jnp.minimum(gates, 0.0) - jnp.log1p(jnp.exp(-jnp.abs(gates)))
        square = (PROPS, PROPS)
        older = lax.broadcasted_iota(jnp.int32, square, 0)
        younger = lax.broadcasted_iota(jnp.int32, square, 1)
        linked = (older == v_par[pl.ds(mine, 1), :]) | (older == younger)
        up = linked.astype(F32)
        for _ in range(5):
            closed = up.astype(BF16)
            up = jnp.minimum(jnp.dot(closed, closed, preferred_element_type=F32), 1.0)
        eye = (older == younger).astype(F32)
        ancestry = nt_dot(eye.astype(BF16), up.astype(BF16))
        path_rows = jnp.dot(
            log_gates[:, :PROPS], up, preferred_element_type=F32, precision=lax.Precision.HIGHEST
        )

        arrived(s_k, r_k, k_send, k_recv)
        new_keys = r_k[0]
        for i in range(1, NKV):
            new_keys = new_keys + r_k[i]
        new_keys = (inverse * new_keys).astype(BF16)
        q = by_head(g_q[mine].astype(F32) * (HEAD_DIM**-0.5), wide).astype(BF16)
        scores = nt_dot(q, new_keys)
        parts = []
        for h in range(HEADS):
            part = scores[h * PROPS : (h + 1) * PROPS] - path_rows[h : h + 1]
            parts.append(jnp.where(ancestry > 0.5, part, NEG))
        scores = jnp.concatenate(parts, axis=0)
        tree_top = jnp.max(scores, axis=1, keepdims=True)
        weights = jnp.exp(scores - tree_top)
        tree_total = jnp.sum(weights, axis=1, keepdims=True)
        arrived(s_v, r_v, v_send, v_recv)
        new_values = r_v[0].astype(F32)
        for i in range(1, NKV):
            new_values = new_values + r_v[i].astype(F32)
        new_values = (inverse * new_values).astype(BF16)
        tree_mix = diagonal(
            jnp.dot(weights.astype(BF16), new_values, preferred_element_type=F32), lane
        )
        tree_stats = stat_rows(tree_top, tree_total)

        arrived(s_stat, r_stat, y_send, y_recv)
        stats = [r_stat[i] for i in range(NKV)] + [tree_stats]
        best = functools.reduce(jnp.maximum, stats)
        factors = [jnp.exp(s - best) for s in stats]
        denominator = functools.reduce(
            jnp.add, [pltpu.roll(s, HEADS, 0) * f for s, f in zip(stats, factors)]
        )
        under = 1.0 / denominator
        columns = jnp.concatenate([f * under for f in factors[:NKV]], axis=0).T[:PROPS]
        tree_columns = jnp.concatenate(
            [factors[NKV] * under, jnp.zeros((LANES - FEW, LANES), F32)], axis=0
        ).T[:PROPS]
        attended = tree_mix * spread([tree_columns[:, h : h + 1] for h in range(HEADS)], lane)
        arrived(s_mix, r_mix, m_send, m_recv)
        for i in range(NKV):
            shares = [columns[:, FEW * i + h : FEW * i + h + 1] for h in range(HEADS)]
            attended = attended + r_mix[i].astype(F32) * spread(shares, lane)

        @pl.when(out_place != 1)
        def _():
            s_att[...] = attended.astype(BF16)

            for distance in FAR_FIRST:
                whole_copy(distance).start()

            @pl.when(tp != whole_to)
            def _():
                whole_copy((0, 0)).start()

            @pl.when(tp == whole_to)
            def _():
                r_att[tp] = s_att[...]

        @pl.when(out_place == 1)
        def _():
            s_half[0] = attended[:HALF].astype(BF16)
            s_half[1] = attended[PROPS - HALF :].astype(BF16)

            for distance in FAR_FIRST:
                half_copy(distance, 0).start()
                half_copy(distance, 1).start()
            for c in range(2):

                @pl.when(tp != 2 * out_group + c)
                def _():
                    half_copy((0, 0), c).start()

                @pl.when(tp == 2 * out_group + c)
                def _():
                    r_half[tp] = s_half[c]

    def scattered():
        @pl.when(is_whole)
        def _():
            for distance in FAR_FIRST:
                whole_copy(distance).wait_send()

            @pl.when(tp != whole_to)
            def _():
                whole_copy((0, 0)).wait_send()

        @pl.when(is_half)
        def _():
            for c in range(2):
                for distance in FAR_FIRST:
                    half_copy(distance, c).wait_send()

                @pl.when(tp != 2 * out_group + c)
                def _():
                    half_copy((0, 0), c).wait_send()

    lax.fori_loop(1, NTP, weight_arrived, 0)
    for wait in pending:
        wait()

    for group in range(NTP):

        @pl.when((sources[0] != kv) | (tp != group))
        def _():
            pltpu.make_async_remote_copy(
                src_ref=s_att,
                dst_ref=r_att.at[group],
                send_sem=a_send.at[0],
                recv_sem=a_recv.at[group],
                device_id={"kv": sources[0], "tp": group},
                device_id_type=MESH,
            ).wait_recv()

        @pl.when((sources[1] != kv) | (tp != group))
        def _():
            pltpu.make_async_remote_copy(
                src_ref=s_half.at[0],
                dst_ref=r_half.at[group],
                send_sem=a_send.at[0],
                recv_sem=a_recv.at[NTP + group],
                device_id={"kv": sources[1], "tp": group},
                device_id_type=MESH,
            ).wait_recv()

    mixed = jnp.zeros((PROPS + HALF, COLS), F32)
    for group in range(NTP):
        whole, half = r_att[group].astype(F32), r_half[group].astype(F32)
        both = jnp.where(
            odd == 1,
            jnp.concatenate([half, whole], axis=0),
            jnp.concatenate([whole, half], axis=0),
        )
        term = jnp.dot(both.astype(BF16), v_wo[group], preferred_element_type=F32)
        mixed = mixed + term.astype(BF16).astype(F32)
    out_ref[...] = jnp.where(
        odd == 1, mixed[PROPS + HALF - OUT_ROWS :], mixed[:OUT_ROWS]
    ).astype(BF16)
    scattered()


def body(
    tokens,
    norm_gain,
    query_weight,
    key_weight,
    value_weight,
    gate_weight,
    gate_bias,
    out_weight,
    cache_keys,
    cache_values,
    cache_decay,
    lengths,
    parents,
):
    anywhere = pl.BlockSpec(memory_space=pl.ANY)
    vector = pl.BlockSpec(memory_space=pltpu.VMEM)
    dma = pltpu.SemaphoreType.DMA
    return pl.pallas_call(
        kernel,
        out_shape=jax.ShapeDtypeStruct((OUT_ROWS, COLS), BF16),
        in_specs=[anywhere] * 13,
        out_specs=vector,
        scratch_shapes=[
            pltpu.VMEM((ROWS, COLS), BF16),
            pltpu.VMEM((1, COLS), F32),
            pltpu.VMEM((COLS, COLS), BF16),
            pltpu.VMEM((COLS, COLS), BF16),
            pltpu.VMEM((COLS, COLS), BF16),
            pltpu.VMEM((32, COLS), BF16),
            pltpu.VMEM((NTP, COLS, COLS), BF16),
            pltpu.VMEM((SEQS, POS, COLS), BF16),
            pltpu.VMEM((SEQS, POS, COLS), BF16),
            pltpu.VMEM((SEQS, HEADS, POS), F32),
            pltpu.SMEM((SEQS,), jnp.int32),
            pltpu.SMEM((NTP * HEADS,), F32),
            pltpu.VMEM((SEQS, PROPS), jnp.int32),
            pltpu.VMEM((SEQS, PROPS, COLS), F32),
            pltpu.VMEM((SEQS, 1, LANES), F32),
            pltpu.VMEM((SEQS, FEW, LANES), F32),
            pltpu.VMEM((SEQS, PROPS, COLS), F32),
            pltpu.VMEM((SEQS, PROPS, COLS), BF16),
            pltpu.VMEM((NKV, PROPS, COLS), F32),
            pltpu.VMEM((NKV, 1, LANES), F32),
            pltpu.VMEM((NKV, FEW, LANES), F32),
            pltpu.VMEM((NKV, PROPS, COLS), F32),
            pltpu.VMEM((NKV, PROPS, COLS), BF16),
            pltpu.VMEM((SEQS, PROPS, COLS), BF16),
            pltpu.VMEM((1, LANES), F32),
            pltpu.VMEM((PROPS, LANES), F32),
            pltpu.VMEM((SEQS, PROPS, COLS), BF16),
            pltpu.VMEM((SEQS, FEW, LANES), F32),
            pltpu.VMEM((NKV, PROPS, COLS), BF16),
            pltpu.VMEM((NKV, FEW, LANES), F32),
            pltpu.VMEM((PROPS, COLS), BF16),
            pltpu.VMEM((2, HALF, COLS), BF16),
            pltpu.VMEM((NTP, PROPS, COLS), BF16),
            pltpu.VMEM((NTP, HALF, COLS), BF16),
            dma((13,)),
            dma((SEQS,)),
            dma((NKV,)),
            dma((SEQS,)),
            dma((NKV,)),
            dma((SEQS,)),
            dma((NKV,)),
            dma((SEQS,)),
            dma((NKV,)),
            dma((SEQS,)),
            dma((NKV,)),
            dma((NKV,)),
            dma((SEQS,)),
            dma((SEQS,)),
            dma((NKV,)),
            dma((SEQS,)),
            dma((NKV,)),
            dma((2 * NKV,)),
            dma((2 * NTP,)),
            dma((NTP,)),
            dma((NTP,)),
        ],
        compiler_params=pltpu.CompilerParams(
            collective_id=0, has_side_effects=True, vmem_limit_bytes=60 * 1024 * 1024
        ),
        name="tree_attention",
    )(
        tokens,
        norm_gain.reshape(1, -1),
        query_weight,
        key_weight,
        value_weight,
        gate_weight.T,
        gate_bias,
        out_weight,
        cache_keys,
        cache_values,
        cache_decay,
        lengths,
        parents,
    )


def solution(mesh):
    in_specs = (
        P(None, "kv"),
        P("kv"),
        P("kv", "tp"),
        P("kv", "tp"),
        P("kv", "tp"),
        P(),
        P(),
        P("tp", "kv"),
        P(None, "kv", "tp"),
        P(None, "kv", "tp"),
        P(None, "tp", "kv"),
        P(),
        P(),
    )
    out_specs = P("tp", "kv")
    return jax.shard_map(body, mesh=mesh, in_specs=in_specs, out_specs=out_specs, check_vma=False)
```

```python
import functools

import jax
import jax.numpy as jnp
from jax import lax
from jax.experimental import pallas as pl
from jax.experimental.pallas import tpu as pltpu
from jax.sharding import PartitionSpec as P

MESH = pl.DeviceIdType.MESH
F32 = jnp.float32
BF16 = jnp.bfloat16
NKV = 16
NTP = 8
SEQS = 12
PROPS = 24
POS = 384
HEADS = 4
HEAD_DIM = 64
COLS = HEADS * HEAD_DIM
ROWS = SEQS * PROPS
OUT_ROWS = ROWS // NTP
LANES = 128
FULL_WIDTH = 4096.0
NEG = -1e30
GROUP = 3
HALF = 16
FEW = 8
IN_ORDER = (0, 1, 4, 3, 2, 5, 8, 7, 6, 9, 12, 11, 10, 13, 15, 14)
FAR_FIRST = sorted(
    [(z, x) for z in range(4) for x in range(4) if z or x],
    key=lambda d: -sum(min(n, 4 - n) for n in d),
)


def nt_dot(a, b, precision=None):
    return lax.dot_general(
        a, b, (((1,), (1,)), ((), ())), preferred_element_type=F32, precision=precision
    )


def below(value, count):
    return jnp.where(value >= count, value - count, value)


def third(value):
    part = (
        jnp.where(value >= 3, 1, 0) + jnp.where(value >= 6, 1, 0) + jnp.where(value >= 9, 1, 0)
    )
    return part, value - 3 * part


def owner_of(seq):
    group, place = third(seq)
    row = below(group + 4 - place, 4)
    return 4 * row + place + jnp.where(place >= row, 1, 0)


def seq_at(index):
    row, place = third(index)
    return 3 * below(row + place, 4) + place


def spread(columns, lane):
    halves = []
    for pair in range(2):
        halves.append(jnp.where(lane < HEAD_DIM, columns[2 * pair], columns[2 * pair + 1]))
    return jnp.concatenate(halves, axis=1)


def diagonal(stacked, lane):
    halves = []
    for pair in range(2):
        even = stacked[(2 * pair) * PROPS : (2 * pair + 1) * PROPS, pair * LANES : (pair + 1) * LANES]
        odd = stacked[
            (2 * pair + 1) * PROPS : (2 * pair + 2) * PROPS, pair * LANES : (pair + 1) * LANES
        ]
        halves.append(jnp.where(lane < HEAD_DIM, even, odd))
    return jnp.concatenate(halves, axis=1)


def by_head(q, wide):
    parts = [
        jnp.where((wide >= h * HEAD_DIM) & (wide < (h + 1) * HEAD_DIM), q, 0.0)
        for h in range(HEADS)
    ]
    return jnp.concatenate(parts, axis=0)


def kernel(
    tokens,
    gain,
    wq,
    wk,
    wv,
    gw,
    bias,
    wo,
    ckeys,
    cvals,
    cdecay,
    lengths,
    parents,
    out_ref,
    v_tok,
    v_gain,
    v_wq,
    v_wk,
    v_wv,
    v_gw,
    v_wo,
    v_ck,
    v_cv,
    v_cd,
    v_len,
    v_bias,
    v_par,
    s_q,
    s_sq,
    s_k,
    s_v,
    r_q,
    r_sq,
    r_k,
    r_v,
    g_q,
    i_row,
    i_col,
    s_mix,
    s_stat,
    r_mix,
    r_stat,
    s_att,
    s_half,
    r_att,
    r_half,
    load_sem,
    q_send,
    q_recv,
    z_send,
    z_recv,
    k_send,
    k_recv,
    v_send,
    v_recv,
    gq_send,
    gq_recv,
    m_send,
    m_recv,
    y_send,
    y_recv,
    a_send,
    a_recv,
    w_send,
    w_recv,
):
    kv = lax.axis_index("kv")
    tp = lax.axis_index("tp")
    row, column = lax.div(kv, 4), lax.rem(kv, 4)
    is_owner = row != column
    index = 3 * row + jnp.minimum(jnp.where(column > row, column - 1, column), 2)
    mine = seq_at(index)
    out_group, out_place = third(mine)
    whole_to = 2 * out_group + jnp.where(out_place == 2, 1, 0)
    is_whole = is_owner & (out_place != 1)
    is_half = is_owner & (out_place == 1)
    out_third = lax.div(tp, 2)
    odd = tp - 2 * out_third
    sources = [owner_of(3 * out_third + 2 * odd), owner_of(3 * out_third + 1)]

    gate_cols = gw.at[:, pl.ds(pl.multiple_of(kv * COLS, COLS), COLS)]
    loads = [
        pltpu.make_async_copy(src, dst, load_sem.at[n])
        for n, (src, dst) in enumerate(
            [
                (tokens, v_tok),
                (gain, v_gain),
                (wq, v_wq),
                (gate_cols, v_gw),
                (wk, v_wk),
                (wv, v_wv),
                (ckeys, v_ck),
                (cdecay, v_cd),
                (cvals, v_cv),
                (wo, v_wo.at[tp]),
                (lengths, v_len),
                (bias, v_bias),
                (parents, v_par),
            ]
        )
    ]
    for load in loads:
        load.start()
    l_tok, l_gain, l_wq, l_gw, l_wk, l_wv, l_ck, l_cd, l_cv, l_wo, l_len, l_bias, l_par = loads

    barrier = pltpu.get_barrier_semaphore()
    for r in range(1, NKV):
        pl.semaphore_signal(
            barrier, inc=1, device_id={"kv": below(kv + r, NKV)}, device_id_type=MESH
        )
    for r in range(1, NTP):
        pl.semaphore_signal(
            barrier, inc=1, device_id={"tp": below(tp + r, NTP)}, device_id_type=MESH
        )
    greeted = NKV - 1 + NTP - 1
    greeted = greeted + jnp.where(is_whole, NKV, 0) + jnp.where(is_half, 2 * NKV, 0)
    greeted = greeted - jnp.where(is_whole & (tp == whole_to), 1, 0)
    greeted = greeted - jnp.where(is_half & (out_third == out_group), 1, 0)
    for source in sources:
        for group in range(NTP):

            @pl.when((source != kv) | (tp != group))
            def _():
                pl.semaphore_signal(
                    barrier, inc=1, device_id={"kv": source, "tp": group}, device_id_type=MESH
                )

    lane = lax.broadcasted_iota(jnp.int32, (PROPS, LANES), 1)
    wide = lax.broadcasted_iota(jnp.int32, (PROPS, COLS), 1)

    def exchange(src, dst, send, recv, seq):
        return pltpu.make_async_remote_copy(
            src_ref=src.at[seq],
            dst_ref=dst.at[kv],
            send_sem=send.at[seq],
            recv_sem=recv.at[kv],
            device_id={"kv": owner_of(seq)},
            device_id_type=MESH,
        )

    def at_distance(z, x):
        return below(row + z, 4), below(column + x, 4)

    def to_owners(src, dst, send, recv):
        for distance in FAR_FIRST:
            z, x = at_distance(*distance)

            @pl.when(z != x)
            def _():
                seq = seq_at(3 * z + jnp.where(x > z, x - 1, x))
                exchange(src, dst, send, recv, seq).start()

    def sent_to_owners(src, dst, send, recv):
        for seq in range(SEQS):

            @pl.when(owner_of(seq) != kv)
            def _():
                exchange(src, dst, send, recv, seq).wait_send()

    def arrived(src, dst, send, recv):
        def step(i, carry):
            @pl.when(i != kv)
            def _():
                pltpu.make_async_remote_copy(
                    src_ref=src.at[0],
                    dst_ref=dst.at[i],
                    send_sem=send.at[0],
                    recv_sem=recv.at[i],
                    device_id={"kv": i},
                    device_id_type=MESH,
                ).wait_recv()

            return carry

        lax.fori_loop(0, NKV, step, 0)

    def gather_copy(buf, send, recv, peer, slot, seq):
        return pltpu.make_async_remote_copy(
            src_ref=buf.at[seq],
            dst_ref=buf.at[seq],
            send_sem=send.at[slot],
            recv_sem=recv.at[seq],
            device_id={"kv": peer},
            device_id_type=MESH,
        )

    def to_all(buf, send, recv):
        for r in range(1, NKV):
            gather_copy(buf, send, recv, below(kv + r, NKV), r, mine).start()

    def sent_to_all(buf, send, recv):
        for r in range(1, NKV):
            gather_copy(buf, send, recv, below(kv + r, NKV), r, mine).wait_send()

    def whole_copy(to):
        return pltpu.make_async_remote_copy(
            src_ref=s_att,
            dst_ref=r_att.at[tp],
            send_sem=a_send.at[to],
            recv_sem=a_recv.at[tp],
            device_id={"kv": to, "tp": whole_to},
            device_id_type=MESH,
        )

    def half_copy(to, c):
        return pltpu.make_async_remote_copy(
            src_ref=s_half.at[c],
            dst_ref=r_half.at[tp],
            send_sem=a_send.at[NKV * c + to],
            recv_sem=a_recv.at[NTP + tp],
            device_id={"kv": to, "tp": 2 * out_group + c},
            device_id_type=MESH,
        )

    def await_seq(buf, send, recv, seq):
        @pl.when(owner_of(seq) != kv)
        def _():
            gather_copy(buf, send, recv, owner_of(seq), 0, seq).wait_recv()

    pending = []

    l_tok.wait()
    l_gain.wait()
    x = v_tok[...].astype(F32)
    normed = (x * v_gain[...]).astype(BF16)
    l_wq.wait()
    s_q[...] = jnp.dot(normed, v_wq[...], preferred_element_type=F32).reshape(SEQS, PROPS, COLS)
    squares = x * x
    high = squares.astype(BF16)
    low = (squares - high.astype(F32)).astype(BF16)
    ones = jnp.ones((16, COLS), BF16)
    square_rows = nt_dot(ones, high) + nt_dot(ones, low)
    l_gw.wait()
    pick_row = lax.broadcasted_iota(jnp.int32, (16, 32), 0)
    pick_col = lax.broadcasted_iota(jnp.int32, (16, 32), 1)
    pick = (pick_col == tp * HEADS + pick_row) & (pick_row < HEADS)
    own_gates = jnp.dot(
        pick.astype(F32).astype(BF16), v_gw[...], preferred_element_type=F32
    ).astype(BF16)
    rows = jnp.where(
        lax.broadcasted_iota(jnp.int32, (FEW, ROWS), 0) < HEADS,
        nt_dot(own_gates, normed)[:FEW],
        square_rows[:FEW],
    )
    rows = jnp.concatenate([rows, jnp.zeros((FEW, 3 * LANES - ROWS), F32)], axis=1)
    wide_row = lax.broadcasted_iota(jnp.int32, rows.shape, 0)
    placed = rows
    for h in range(1, HEADS + 1):
        placed = jnp.where(wide_row == h, pltpu.roll(rows, h * PROPS, 1), placed)
    few_row = lax.broadcasted_iota(jnp.int32, (FEW, LANES), 0)
    few_lane = lax.broadcasted_iota(jnp.int32, (FEW, LANES), 1) - PROPS * few_row
    kept = (few_lane >= 0) & (few_lane < PROPS) & (few_row <= HEADS)
    for seq in range(SEQS):
        shift = (3 * LANES - seq * PROPS) % (3 * LANES)
        turned = pltpu.roll(placed, shift, 1) if shift else placed
        s_sq[seq] = jnp.sum(jnp.where(kept, turned[:, :LANES], 0.0), axis=0, keepdims=True)

    pl.semaphore_wait(barrier, greeted)
    to_owners(s_sq, r_sq, z_send, z_recv)
    to_owners(s_q, r_q, q_send, q_recv)
    pending.append(lambda: sent_to_owners(s_sq, r_sq, z_send, z_recv))
    pending.append(lambda: sent_to_owners(s_q, r_q, q_send, q_recv))

    def weight_copy(to, source):
        return pltpu.make_async_remote_copy(
            src_ref=v_wo.at[source],
            dst_ref=v_wo.at[source],
            send_sem=w_send.at[to],
            recv_sem=w_recv.at[source],
            device_id={"tp": to},
            device_id_type=MESH,
        )

    def send_weight(r, carry):
        weight_copy(below(tp + r, NTP), tp).start()
        return carry

    def weight_sent(r, carry):
        weight_copy(below(tp + r, NTP), tp).wait_send()
        return carry

    def weight_arrived(r, carry):
        source = below(tp + r, NTP)
        weight_copy(source, source).wait_recv()
        return carry

    l_wo.wait()
    lax.fori_loop(1, NTP, send_weight, 0)
    pending.append(lambda: lax.fori_loop(1, NTP, weight_sent, 0))

    l_wk.wait()
    s_k[...] = jnp.dot(normed, v_wk[...], preferred_element_type=F32).reshape(SEQS, PROPS, COLS)
    l_wv.wait()
    new = jnp.dot(normed, v_wv[...], preferred_element_type=F32)
    s_v[...] = new.astype(BF16).reshape(SEQS, PROPS, COLS)

    @pl.when(is_owner)
    def _():
        r_q[kv] = s_q[mine]
        r_sq[kv] = s_sq[mine]
        arrived(s_sq, r_sq, z_send, z_recv)
        summed = r_sq[0]
        for i in range(1, NKV):
            summed = summed + r_sq[i]
        i_row[...] = summed
        on_diagonal = lane == HEADS * PROPS + lax.broadcasted_iota(jnp.int32, (PROPS, LANES), 0)
        own_squares = jnp.sum(jnp.where(on_diagonal, summed, 0.0), axis=1, keepdims=True)
        inverse = lax.rsqrt(own_squares / FULL_WIDTH + 1e-6)
        i_col[...] = jnp.broadcast_to(inverse, (PROPS, LANES))
        arrived(s_q, r_q, q_send, q_recv)
        total = r_q[0]
        for i in range(1, NKV):
            total = total + r_q[i]
        g_q[mine] = (inverse * total).astype(BF16)
        to_all(g_q, gq_send, gq_recv)

    pending.append(lambda: pl.when(is_owner)(lambda: sent_to_all(g_q, gq_send, gq_recv)))
    to_owners(s_k, r_k, k_send, k_recv)
    pending.append(lambda: sent_to_owners(s_k, r_k, k_send, k_recv))
    to_owners(s_v, r_v, v_send, v_recv)
    pending.append(lambda: sent_to_owners(s_v, r_v, v_send, v_recv))

    l_ck.wait()
    l_cd.wait()
    l_len.wait()
    l_bias.wait()
    l_par.wait()
    l_cv.wait()
    position = kv * POS + lax.broadcasted_iota(jnp.int32, (1, POS), 1)

    own_lane = wide - lax.broadcasted_iota(jnp.int32, (PROPS, COLS), 0)

    def stat_row(top, total):
        stats = jnp.zeros((PROPS, COLS), F32)
        for h in range(HEADS):
            own = slice(h * PROPS, (h + 1) * PROPS)
            stats = jnp.where(own_lane == h * PROPS, top[own], stats)
            stats = jnp.where(own_lane == (HEADS + h) * PROPS, total[own], stats)
        return jnp.sum(stats, axis=0, keepdims=True)

    def attend(seq):
        q = by_head(g_q[seq].astype(F32) * (HEAD_DIM**-0.5), wide).astype(BF16)
        scores = nt_dot(q, v_ck[seq])
        live = position < v_len[seq]
        parts = []
        for h in range(HEADS):
            decay = jnp.where(live, v_cd[seq, h : h + 1, :], NEG)
            parts.append(scores[h * PROPS : (h + 1) * PROPS] + decay)
        scores = jnp.concatenate(parts, axis=0)
        top = jnp.max(scores, axis=1, keepdims=True)
        weights = jnp.exp(scores - top)
        total = jnp.sum(weights, axis=1, keepdims=True)
        mix = jnp.dot(weights.astype(BF16), v_cv[seq], preferred_element_type=F32)
        s_mix[seq] = diagonal(mix, lane).astype(BF16)
        s_stat[seq] = stat_row(top, total)

    def attend_group(j, carry):
        seqs = [seq_at(below(index + SEQS - j * GROUP - u, SEQS)) for u in range(GROUP)]
        for seq in seqs:
            await_seq(g_q, gq_send, gq_recv, seq)
        for seq in seqs:
            attend(seq)
        for seq in seqs:

            @pl.when(owner_of(seq) != kv)
            def _():
                exchange(s_stat, r_stat, y_send, y_recv, seq).start()
                exchange(s_mix, r_mix, m_send, m_recv, seq).start()

        return carry

    lax.fori_loop(0, SEQS // GROUP, attend_group, 0)

    pending.append(lambda: sent_to_owners(s_mix, r_mix, m_send, m_recv))
    pending.append(lambda: sent_to_owners(s_stat, r_stat, y_send, y_recv))
    @pl.when(is_owner)
    def _():
        r_k[kv] = s_k[mine]
        r_v[kv] = s_v[mine]
        r_mix[kv] = s_mix[mine]
        r_stat[kv] = s_stat[mine]
        inverse = i_col[:, 0:1]
        head_row = lax.broadcasted_iota(jnp.int32, (FEW, LANES), 0)
        shift = jnp.zeros((FEW, LANES), F32)
        for h in range(HEADS):
            shift = jnp.where(head_row == h, v_bias[tp * HEADS + h], shift)
        summed = jnp.broadcast_to(i_row[...], (FEW, LANES))
        gates = summed
        for h in range(1, HEADS):
            gates = jnp.where(head_row == h, pltpu.roll(summed, LANES - h * PROPS, 1), gates)
        own_squares = pltpu.roll(summed, LANES - HEADS * PROPS, 1)
        gates = lax.rsqrt(own_squares / FULL_WIDTH + 1e-6) * gates + shift
        log_gates = jnp.minimum(gates, 0.0) - jnp.log1p(jnp.exp(-jnp.abs(gates)))
        square = (PROPS, PROPS)
        older = lax.broadcasted_iota(jnp.int32, square, 0)
        younger = lax.broadcasted_iota(jnp.int32, square, 1)
        linked = (older == v_par[pl.ds(mine, 1), :]) | (older == younger)
        up = linked.astype(F32)
        for _ in range(5):
            closed = up.astype(BF16)
            up = jnp.minimum(jnp.dot(closed, closed, preferred_element_type=F32), 1.0)
        eye = (older == younger).astype(F32)
        ancestry = nt_dot(eye.astype(BF16), up.astype(BF16))
        path_rows = jnp.dot(
            log_gates[:, :PROPS], up, preferred_element_type=F32, precision=lax.Precision.HIGHEST
        )

        arrived(s_k, r_k, k_send, k_recv)
        new_keys = r_k[0]
        for i in range(1, NKV):
            new_keys = new_keys + r_k[i]
        new_keys = (inverse * new_keys).astype(BF16)
        q = by_head(g_q[mine].astype(F32) * (HEAD_DIM**-0.5), wide).astype(BF16)
        scores = nt_dot(q, new_keys)
        parts = []
        for h in range(HEADS):
            part = scores[h * PROPS : (h + 1) * PROPS] - path_rows[h : h + 1]
            parts.append(jnp.where(ancestry > 0.5, part, NEG))
        scores = jnp.concatenate(parts, axis=0)
        tree_top = jnp.max(scores, axis=1, keepdims=True)
        weights = jnp.exp(scores - tree_top)
        tree_total = jnp.sum(weights, axis=1, keepdims=True)
        arrived(s_v, r_v, v_send, v_recv)
        new_values = r_v[0].astype(F32)
        for i in range(1, NKV):
            new_values = new_values + r_v[i].astype(F32)
        new_values = (inverse * new_values).astype(BF16)
        tree_mix = diagonal(
            jnp.dot(weights.astype(BF16), new_values, preferred_element_type=F32), lane
        )
        tree_stats = stat_row(tree_top, tree_total)

        arrived(s_stat, r_stat, y_send, y_recv)
        stats = [r_stat[i] for i in range(NKV)] + [tree_stats]
        best = functools.reduce(jnp.maximum, stats)
        factors = [jnp.exp(s - best) for s in stats]
        denominator = functools.reduce(
            jnp.add,
            [pltpu.roll(s, COLS - HEADS * PROPS, 1) * f for s, f in zip(stats, factors)],
        )
        under = 1.0 / denominator
        shares = jnp.concatenate(
            [(f * under)[:, :LANES] for f in factors]
            + [jnp.zeros((LANES - NKV - 1, LANES), F32)],
            axis=0,
        )
        used = lax.broadcasted_iota(jnp.int32, shares.shape, 1) < HEADS * PROPS
        shares = jnp.where(used, shares, 0.0).T

        def share_of(i):
            return spread(
                [shares[h * PROPS : (h + 1) * PROPS, i : i + 1] for h in range(HEADS)], lane
            )

        attended = tree_mix * share_of(NKV)
        arrived(s_mix, r_mix, m_send, m_recv)
        for i in range(NKV):
            attended = attended + r_mix[i].astype(F32) * share_of(i)

        @pl.when(out_place != 1)
        def _():
            s_att[...] = attended.astype(BF16)

            for to in IN_ORDER:

                @pl.when((kv != to) | (tp != whole_to))
                def _():
                    whole_copy(to).start()

            @pl.when(tp == whole_to)
            def _():
                r_att[tp] = s_att[...]

        @pl.when(out_place == 1)
        def _():
            s_half[0] = attended[:HALF].astype(BF16)
            s_half[1] = attended[PROPS - HALF :].astype(BF16)

            for to in IN_ORDER:
                for c in range(2):

                    @pl.when((kv != to) | (tp != 2 * out_group + c))
                    def _():
                        half_copy(to, c).start()

            for c in range(2):

                @pl.when(tp == 2 * out_group + c)
                def _():
                    r_half[tp] = s_half[c]

    def scattered():
        for to in IN_ORDER:

            @pl.when(is_whole & ((kv != to) | (tp != whole_to)))
            def _():
                whole_copy(to).wait_send()

            for c in range(2):

                @pl.when(is_half & ((kv != to) | (tp != 2 * out_group + c)))
                def _():
                    half_copy(to, c).wait_send()

    lax.fori_loop(1, NTP, weight_arrived, 0)
    for wait in pending:
        wait()

    for group in range(NTP):

        @pl.when((sources[0] != kv) | (tp != group))
        def _():
            pltpu.make_async_remote_copy(
                src_ref=s_att,
                dst_ref=r_att.at[group],
                send_sem=a_send.at[0],
                recv_sem=a_recv.at[group],
                device_id={"kv": sources[0], "tp": group},
                device_id_type=MESH,
            ).wait_recv()

        @pl.when((sources[1] != kv) | (tp != group))
        def _():
            pltpu.make_async_remote_copy(
                src_ref=s_half.at[0],
                dst_ref=r_half.at[group],
                send_sem=a_send.at[0],
                recv_sem=a_recv.at[NTP + group],
                device_id={"kv": sources[1], "tp": group},
                device_id_type=MESH,
            ).wait_recv()

    mixed = jnp.zeros((PROPS + HALF, COLS), F32)
    for group in range(NTP):
        whole, half = r_att[group].astype(F32), r_half[group].astype(F32)
        both = jnp.where(
            odd == 1,
            jnp.concatenate([half, whole], axis=0),
            jnp.concatenate([whole, half], axis=0),
        )
        term = jnp.dot(both.astype(BF16), v_wo[group], preferred_element_type=F32)
        mixed = mixed + term.astype(BF16).astype(F32)
    out_ref[...] = jnp.where(
        odd == 1, mixed[PROPS + HALF - OUT_ROWS :], mixed[:OUT_ROWS]
    ).astype(BF16)
    scattered()


def body(
    tokens,
    norm_gain,
    query_weight,
    key_weight,
    value_weight,
    gate_weight,
    gate_bias,
    out_weight,
    cache_keys,
    cache_values,
    cache_decay,
    lengths,
    parents,
):
    anywhere = pl.BlockSpec(memory_space=pl.ANY)
    vector = pl.BlockSpec(memory_space=pltpu.VMEM)
    dma = pltpu.SemaphoreType.DMA
    return pl.pallas_call(
        kernel,
        out_shape=jax.ShapeDtypeStruct((OUT_ROWS, COLS), BF16),
        in_specs=[anywhere] * 13,
        out_specs=vector,
        scratch_shapes=[
            pltpu.VMEM((ROWS, COLS), BF16),
            pltpu.VMEM((1, COLS), F32),
            pltpu.VMEM((COLS, COLS), BF16),
            pltpu.VMEM((COLS, COLS), BF16),
            pltpu.VMEM((COLS, COLS), BF16),
            pltpu.VMEM((32, COLS), BF16),
            pltpu.VMEM((NTP, COLS, COLS), BF16),
            pltpu.VMEM((SEQS, POS, COLS), BF16),
            pltpu.VMEM((SEQS, POS, COLS), BF16),
            pltpu.VMEM((SEQS, HEADS, POS), F32),
            pltpu.SMEM((SEQS,), jnp.int32),
            pltpu.SMEM((NTP * HEADS,), F32),
            pltpu.VMEM((SEQS, PROPS), jnp.int32),
            pltpu.VMEM((SEQS, PROPS, COLS), F32),
            pltpu.VMEM((SEQS, 1, LANES), F32),
            pltpu.VMEM((SEQS, PROPS, COLS), F32),
            pltpu.VMEM((SEQS, PROPS, COLS), BF16),
            pltpu.VMEM((NKV, PROPS, COLS), F32),
            pltpu.VMEM((NKV, 1, LANES), F32),
            pltpu.VMEM((NKV, PROPS, COLS), F32),
            pltpu.VMEM((NKV, PROPS, COLS), BF16),
            pltpu.VMEM((SEQS, PROPS, COLS), BF16),
            pltpu.VMEM((1, LANES), F32),
            pltpu.VMEM((PROPS, LANES), F32),
            pltpu.VMEM((SEQS, PROPS, COLS), BF16),
            pltpu.VMEM((SEQS, 1, COLS), F32),
            pltpu.VMEM((NKV, PROPS, COLS), BF16),
            pltpu.VMEM((NKV, 1, COLS), F32),
            pltpu.VMEM((PROPS, COLS), BF16),
            pltpu.VMEM((2, HALF, COLS), BF16),
            pltpu.VMEM((NTP, PROPS, COLS), BF16),
            pltpu.VMEM((NTP, HALF, COLS), BF16),
            dma((13,)),
            dma((SEQS,)),
            dma((NKV,)),
            dma((SEQS,)),
            dma((NKV,)),
            dma((SEQS,)),
            dma((NKV,)),
            dma((SEQS,)),
            dma((NKV,)),
            dma((NKV,)),
            dma((SEQS,)),
            dma((SEQS,)),
            dma((NKV,)),
            dma((SEQS,)),
            dma((NKV,)),
            dma((2 * NKV,)),
            dma((2 * NTP,)),
            dma((NTP,)),
            dma((NTP,)),
        ],
        compiler_params=pltpu.CompilerParams(
            collective_id=0, has_side_effects=True, vmem_limit_bytes=60 * 1024 * 1024
        ),
        name="tree_attention",
    )(
        tokens,
        norm_gain.reshape(1, -1),
        query_weight,
        key_weight,
        value_weight,
        gate_weight.T,
        gate_bias,
        out_weight,
        cache_keys,
        cache_values,
        cache_decay,
        lengths,
        parents,
    )


def solution(mesh):
    in_specs = (
        P(None, "kv"),
        P("kv"),
        P("kv", "tp"),
        P("kv", "tp"),
        P("kv", "tp"),
        P(),
        P(),
        P("tp", "kv"),
        P(None, "kv", "tp"),
        P(None, "kv", "tp"),
        P(None, "tp", "kv"),
        P(),
        P(),
    )
    out_specs = P("tp", "kv")
    return jax.shard_map(body, mesh=mesh, in_specs=in_specs, out_specs=out_specs, check_vma=False)
```

```python
import functools

import jax
import jax.numpy as jnp
from jax import lax
from jax.experimental import pallas as pl
from jax.experimental.pallas import tpu as pltpu
from jax.sharding import PartitionSpec as P

MESH = pl.DeviceIdType.MESH
F32 = jnp.float32
BF16 = jnp.bfloat16
NKV = 16
NTP = 8
SEQS = 12
PROPS = 24
POS = 384
HEADS = 4
HEAD_DIM = 64
COLS = HEADS * HEAD_DIM
ROWS = SEQS * PROPS
OUT_ROWS = ROWS // NTP
LANES = 128
FULL_WIDTH = 4096.0
NEG = -1e30
GROUP = 3
HALF = 16
FEW = 8
IN_ORDER = (0, 1, 4, 3, 2, 5, 8, 7, 6, 9, 12, 11, 10, 13, 15, 14)
FAR_FIRST = sorted(
    [(z, x) for z in range(4) for x in range(4) if z or x],
    key=lambda d: -sum(min(n, 4 - n) for n in d),
)


def nt_dot(a, b, precision=None):
    return lax.dot_general(
        a, b, (((1,), (1,)), ((), ())), preferred_element_type=F32, precision=precision
    )


def below(value, count):
    return jnp.where(value >= count, value - count, value)


def third(value):
    part = (
        jnp.where(value >= 3, 1, 0) + jnp.where(value >= 6, 1, 0) + jnp.where(value >= 9, 1, 0)
    )
    return part, value - 3 * part


def owner_of(seq):
    group, place = third(seq)
    row = below(group + 4 - place, 4)
    return 4 * row + place + jnp.where(place >= row, 1, 0)


def seq_at(index):
    row, place = third(index)
    return 3 * below(row + place, 4) + place


def spread(columns, lane):
    halves = []
    for pair in range(2):
        halves.append(jnp.where(lane < HEAD_DIM, columns[2 * pair], columns[2 * pair + 1]))
    return jnp.concatenate(halves, axis=1)


def diagonal(stacked, lane):
    halves = []
    for pair in range(2):
        even = stacked[(2 * pair) * PROPS : (2 * pair + 1) * PROPS, pair * LANES : (pair + 1) * LANES]
        odd = stacked[
            (2 * pair + 1) * PROPS : (2 * pair + 2) * PROPS, pair * LANES : (pair + 1) * LANES
        ]
        halves.append(jnp.where(lane < HEAD_DIM, even, odd))
    return jnp.concatenate(halves, axis=1)


def by_head(q, wide):
    parts = [
        jnp.where((wide >= h * HEAD_DIM) & (wide < (h + 1) * HEAD_DIM), q, 0.0)
        for h in range(HEADS)
    ]
    return jnp.concatenate(parts, axis=0)


def kernel(
    tokens,
    gain,
    wq,
    wk,
    wv,
    gw,
    bias,
    wo,
    ckeys,
    cvals,
    cdecay,
    lengths,
    parents,
    out_ref,
    v_tok,
    v_gain,
    v_wq,
    v_wk,
    v_wv,
    v_gw,
    v_wo,
    v_ck,
    v_cv,
    v_cd,
    v_len,
    v_bias,
    v_par,
    s_q,
    s_sq,
    s_k,
    s_v,
    r_q,
    r_sq,
    r_k,
    r_v,
    g_q,
    i_row,
    i_col,
    s_mix,
    s_stat,
    r_mix,
    r_stat,
    s_att,
    s_half,
    r_att,
    r_half,
    load_sem,
    q_send,
    q_recv,
    z_send,
    z_recv,
    k_send,
    k_recv,
    v_send,
    v_recv,
    gq_send,
    gq_recv,
    m_send,
    m_recv,
    y_send,
    y_recv,
    a_send,
    a_recv,
    w_send,
    w_recv,
):
    kv = lax.axis_index("kv")
    tp = lax.axis_index("tp")
    row, column = lax.div(kv, 4), lax.rem(kv, 4)
    is_owner = row != column
    index = 3 * row + jnp.minimum(jnp.where(column > row, column - 1, column), 2)
    mine = seq_at(index)
    out_group, out_place = third(mine)
    whole_to = 2 * out_group + jnp.where(out_place == 2, 1, 0)
    is_whole = is_owner & (out_place != 1)
    is_half = is_owner & (out_place == 1)
    out_third = lax.div(tp, 2)
    odd = tp - 2 * out_third
    sources = [owner_of(3 * out_third + 2 * odd), owner_of(3 * out_third + 1)]

    gate_cols = gw.at[:, pl.ds(pl.multiple_of(kv * COLS, COLS), COLS)]
    loads = [
        pltpu.make_async_copy(src, dst, load_sem.at[n])
        for n, (src, dst) in enumerate(
            [
                (tokens, v_tok),
                (gain, v_gain),
                (wq, v_wq),
                (gate_cols, v_gw),
                (wk, v_wk),
                (wv, v_wv),
                (ckeys, v_ck),
                (cdecay, v_cd),
                (cvals, v_cv),
                (wo, v_wo.at[tp]),
                (lengths, v_len),
                (bias, v_bias),
                (parents, v_par),
            ]
        )
    ]
    for load in loads:
        load.start()
    l_tok, l_gain, l_wq, l_gw, l_wk, l_wv, l_ck, l_cd, l_cv, l_wo, l_len, l_bias, l_par = loads

    barrier = pltpu.get_barrier_semaphore()
    for distance in FAR_FIRST:
        to = 4 * below(row + distance[0], 4) + below(column + distance[1], 4)
        pl.semaphore_signal(barrier, inc=1, device_id={"kv": to}, device_id_type=MESH)
    for r in range(1, NTP):
        pl.semaphore_signal(
            barrier, inc=1, device_id={"tp": below(tp + r, NTP)}, device_id_type=MESH
        )
    greeted = NKV - 1 + NTP - 1
    greeted = greeted + jnp.where(is_whole, NKV, 0) + jnp.where(is_half, 2 * NKV, 0)
    greeted = greeted - jnp.where(is_whole & (tp == whole_to), 1, 0)
    greeted = greeted - jnp.where(is_half & (out_third == out_group), 1, 0)
    for source in sources:
        for group in range(NTP):

            @pl.when((source != kv) | (tp != group))
            def _():
                pl.semaphore_signal(
                    barrier, inc=1, device_id={"kv": source, "tp": group}, device_id_type=MESH
                )

    lane = lax.broadcasted_iota(jnp.int32, (PROPS, LANES), 1)
    wide = lax.broadcasted_iota(jnp.int32, (PROPS, COLS), 1)

    def exchange(src, dst, send, recv, seq):
        return pltpu.make_async_remote_copy(
            src_ref=src.at[seq],
            dst_ref=dst.at[kv],
            send_sem=send.at[seq],
            recv_sem=recv.at[kv],
            device_id={"kv": owner_of(seq)},
            device_id_type=MESH,
        )

    def at_distance(z, x):
        return below(row + z, 4), below(column + x, 4)

    def to_owners(src, dst, send, recv):
        for distance in FAR_FIRST:
            z, x = at_distance(*distance)

            @pl.when(z != x)
            def _():
                seq = seq_at(3 * z + jnp.where(x > z, x - 1, x))
                exchange(src, dst, send, recv, seq).start()

    def sent_to_owners(src, dst, send, recv):
        for seq in range(SEQS):

            @pl.when(owner_of(seq) != kv)
            def _():
                exchange(src, dst, send, recv, seq).wait_send()

    def arrived(src, dst, send, recv):
        def step(i, carry):
            @pl.when(i != kv)
            def _():
                pltpu.make_async_remote_copy(
                    src_ref=src.at[0],
                    dst_ref=dst.at[i],
                    send_sem=send.at[0],
                    recv_sem=recv.at[i],
                    device_id={"kv": i},
                    device_id_type=MESH,
                ).wait_recv()

            return carry

        lax.fori_loop(0, NKV, step, 0)

    def gather_copy(buf, send, recv, peer, slot, seq):
        return pltpu.make_async_remote_copy(
            src_ref=buf.at[seq],
            dst_ref=buf.at[seq],
            send_sem=send.at[slot],
            recv_sem=recv.at[seq],
            device_id={"kv": peer},
            device_id_type=MESH,
        )

    def to_all(buf, send, recv):
        for r in range(1, NKV):
            gather_copy(buf, send, recv, below(kv + r, NKV), r, mine).start()

    def sent_to_all(buf, send, recv):
        for r in range(1, NKV):
            gather_copy(buf, send, recv, below(kv + r, NKV), r, mine).wait_send()

    def whole_copy(to):
        return pltpu.make_async_remote_copy(
            src_ref=s_att,
            dst_ref=r_att.at[tp],
            send_sem=a_send.at[to],
            recv_sem=a_recv.at[tp],
            device_id={"kv": to, "tp": whole_to},
            device_id_type=MESH,
        )

    def half_copy(to, c):
        return pltpu.make_async_remote_copy(
            src_ref=s_half.at[c],
            dst_ref=r_half.at[tp],
            send_sem=a_send.at[NKV * c + to],
            recv_sem=a_recv.at[NTP + tp],
            device_id={"kv": to, "tp": 2 * out_group + c},
            device_id_type=MESH,
        )

    def await_seq(buf, send, recv, seq):
        @pl.when(owner_of(seq) != kv)
        def _():
            gather_copy(buf, send, recv, owner_of(seq), 0, seq).wait_recv()

    pending = []

    l_tok.wait()
    l_gain.wait()
    x = v_tok[...].astype(F32)
    normed = (x * v_gain[...]).astype(BF16)
    l_wq.wait()
    s_q[...] = jnp.dot(normed, v_wq[...], preferred_element_type=F32).reshape(SEQS, PROPS, COLS)
    squares = x * x
    high = squares.astype(BF16)
    low = (squares - high.astype(F32)).astype(BF16)
    ones = jnp.ones((16, COLS), BF16)
    square_rows = nt_dot(ones, high) + nt_dot(ones, low)
    l_gw.wait()
    pick_row = lax.broadcasted_iota(jnp.int32, (16, 32), 0)
    pick_col = lax.broadcasted_iota(jnp.int32, (16, 32), 1)
    pick = (pick_col == tp * HEADS + pick_row) & (pick_row < HEADS)
    own_gates = jnp.dot(
        pick.astype(F32).astype(BF16), v_gw[...], preferred_element_type=F32
    ).astype(BF16)
    rows = jnp.where(
        lax.broadcasted_iota(jnp.int32, (FEW, ROWS), 0) < HEADS,
        nt_dot(own_gates, normed)[:FEW],
        square_rows[:FEW],
    )
    rows = jnp.concatenate([rows, jnp.zeros((FEW, 3 * LANES - ROWS), F32)], axis=1)
    wide_row = lax.broadcasted_iota(jnp.int32, rows.shape, 0)
    placed = rows
    for h in range(1, HEADS + 1):
        placed = jnp.where(wide_row == h, pltpu.roll(rows, h * PROPS, 1), placed)
    few_row = lax.broadcasted_iota(jnp.int32, (FEW, LANES), 0)
    few_lane = lax.broadcasted_iota(jnp.int32, (FEW, LANES), 1) - PROPS * few_row
    kept = (few_lane >= 0) & (few_lane < PROPS) & (few_row <= HEADS)
    for seq in range(SEQS):
        shift = (3 * LANES - seq * PROPS) % (3 * LANES)
        turned = pltpu.roll(placed, shift, 1) if shift else placed
        s_sq[seq] = jnp.sum(jnp.where(kept, turned[:, :LANES], 0.0), axis=0, keepdims=True)

    pl.semaphore_wait(barrier, greeted)
    to_owners(s_sq, r_sq, z_send, z_recv)
    to_owners(s_q, r_q, q_send, q_recv)
    pending.append(lambda: sent_to_owners(s_sq, r_sq, z_send, z_recv))
    pending.append(lambda: sent_to_owners(s_q, r_q, q_send, q_recv))

    def weight_copy(to, source):
        return pltpu.make_async_remote_copy(
            src_ref=v_wo.at[source],
            dst_ref=v_wo.at[source],
            send_sem=w_send.at[to],
            recv_sem=w_recv.at[source],
            device_id={"tp": to},
            device_id_type=MESH,
        )

    def send_weight(r, carry):
        weight_copy(below(tp + r, NTP), tp).start()
        return carry

    def weight_sent(r, carry):
        weight_copy(below(tp + r, NTP), tp).wait_send()
        return carry

    def weight_arrived(r, carry):
        source = below(tp + r, NTP)
        weight_copy(source, source).wait_recv()
        return carry

    l_wo.wait()
    lax.fori_loop(1, NTP, send_weight, 0)
    pending.append(lambda: lax.fori_loop(1, NTP, weight_sent, 0))

    l_wk.wait()
    s_k[...] = jnp.dot(normed, v_wk[...], preferred_element_type=F32).reshape(SEQS, PROPS, COLS)
    l_wv.wait()
    new = jnp.dot(normed, v_wv[...], preferred_element_type=F32)
    s_v[...] = new.astype(BF16).reshape(SEQS, PROPS, COLS)

    @pl.when(is_owner)
    def _():
        r_q[kv] = s_q[mine]
        r_sq[kv] = s_sq[mine]
        arrived(s_sq, r_sq, z_send, z_recv)
        summed = r_sq[0]
        for i in range(1, NKV):
            summed = summed + r_sq[i]
        i_row[...] = summed
        on_diagonal = lane == HEADS * PROPS + lax.broadcasted_iota(jnp.int32, (PROPS, LANES), 0)
        own_squares = jnp.sum(jnp.where(on_diagonal, summed, 0.0), axis=1, keepdims=True)
        inverse = lax.rsqrt(own_squares / FULL_WIDTH + 1e-6)
        i_col[...] = jnp.broadcast_to(inverse, (PROPS, LANES))
        arrived(s_q, r_q, q_send, q_recv)
        total = r_q[0]
        for i in range(1, NKV):
            total = total + r_q[i]
        g_q[mine] = (inverse * total).astype(BF16)
        to_all(g_q, gq_send, gq_recv)

    pending.append(lambda: pl.when(is_owner)(lambda: sent_to_all(g_q, gq_send, gq_recv)))
    to_owners(s_k, r_k, k_send, k_recv)
    pending.append(lambda: sent_to_owners(s_k, r_k, k_send, k_recv))
    to_owners(s_v, r_v, v_send, v_recv)
    pending.append(lambda: sent_to_owners(s_v, r_v, v_send, v_recv))

    l_ck.wait()
    l_cd.wait()
    l_len.wait()
    l_bias.wait()
    l_par.wait()
    l_cv.wait()
    position = kv * POS + lax.broadcasted_iota(jnp.int32, (1, POS), 1)

    own_lane = wide - lax.broadcasted_iota(jnp.int32, (PROPS, COLS), 0)

    def stat_row(top, total):
        stats = jnp.zeros((PROPS, COLS), F32)
        for h in range(HEADS):
            own = slice(h * PROPS, (h + 1) * PROPS)
            stats = jnp.where(own_lane == h * PROPS, top[own], stats)
            stats = jnp.where(own_lane == (HEADS + h) * PROPS, total[own], stats)
        return jnp.sum(stats, axis=0, keepdims=True)

    def attend(seq):
        q = by_head(g_q[seq].astype(F32) * (HEAD_DIM**-0.5), wide).astype(BF16)
        scores = nt_dot(q, v_ck[seq])
        live = position < v_len[seq]
        parts = []
        for h in range(HEADS):
            decay = jnp.where(live, v_cd[seq, h : h + 1, :], NEG)
            parts.append(scores[h * PROPS : (h + 1) * PROPS] + decay)
        scores = jnp.concatenate(parts, axis=0)
        top = jnp.max(scores, axis=1, keepdims=True)
        weights = jnp.exp(scores - top)
        total = jnp.sum(weights, axis=1, keepdims=True)
        mix = jnp.dot(weights.astype(BF16), v_cv[seq], preferred_element_type=F32)
        s_mix[seq] = diagonal(mix, lane).astype(BF16)
        s_stat[seq] = stat_row(top, total)

    def attend_group(j, carry):
        seqs = [seq_at(below(index + SEQS - j * GROUP - u, SEQS)) for u in range(GROUP)]
        for seq in seqs:
            await_seq(g_q, gq_send, gq_recv, seq)
        for seq in seqs:
            attend(seq)
        for seq in seqs:

            @pl.when(owner_of(seq) != kv)
            def _():
                exchange(s_stat, r_stat, y_send, y_recv, seq).start()
                exchange(s_mix, r_mix, m_send, m_recv, seq).start()

        return carry

    lax.fori_loop(0, SEQS // GROUP, attend_group, 0)

    pending.append(lambda: sent_to_owners(s_mix, r_mix, m_send, m_recv))
    pending.append(lambda: sent_to_owners(s_stat, r_stat, y_send, y_recv))
    @pl.when(is_owner)
    def _():
        r_k[kv] = s_k[mine]
        r_v[kv] = s_v[mine]
        r_mix[kv] = s_mix[mine]
        r_stat[kv] = s_stat[mine]
        inverse = i_col[:, 0:1]
        head_row = lax.broadcasted_iota(jnp.int32, (FEW, LANES), 0)
        shift = jnp.zeros((FEW, LANES), F32)
        for h in range(HEADS):
            shift = jnp.where(head_row == h, v_bias[tp * HEADS + h], shift)
        summed = jnp.broadcast_to(i_row[...], (FEW, LANES))
        gates = summed
        for h in range(1, HEADS):
            gates = jnp.where(head_row == h, pltpu.roll(summed, LANES - h * PROPS, 1), gates)
        own_squares = pltpu.roll(summed, LANES - HEADS * PROPS, 1)
        gates = lax.rsqrt(own_squares / FULL_WIDTH + 1e-6) * gates + shift
        log_gates = jnp.minimum(gates, 0.0) - jnp.log1p(jnp.exp(-jnp.abs(gates)))
        square = (PROPS, PROPS)
        older = lax.broadcasted_iota(jnp.int32, square, 0)
        younger = lax.broadcasted_iota(jnp.int32, square, 1)
        linked = (older == v_par[pl.ds(mine, 1), :]) | (older == younger)
        up = linked.astype(F32)
        for _ in range(5):
            closed = up.astype(BF16)
            up = jnp.minimum(jnp.dot(closed, closed, preferred_element_type=F32), 1.0)
        eye = (older == younger).astype(F32)
        ancestry = nt_dot(eye.astype(BF16), up.astype(BF16))
        path_rows = jnp.dot(
            log_gates[:, :PROPS], up, preferred_element_type=F32, precision=lax.Precision.HIGHEST
        )

        arrived(s_k, r_k, k_send, k_recv)
        new_keys = r_k[0]
        for i in range(1, NKV):
            new_keys = new_keys + r_k[i]
        new_keys = (inverse * new_keys).astype(BF16)
        q = by_head(g_q[mine].astype(F32) * (HEAD_DIM**-0.5), wide).astype(BF16)
        scores = nt_dot(q, new_keys)
        parts = []
        for h in range(HEADS):
            part = scores[h * PROPS : (h + 1) * PROPS] - path_rows[h : h + 1]
            parts.append(jnp.where(ancestry > 0.5, part, NEG))
        scores = jnp.concatenate(parts, axis=0)
        tree_top = jnp.max(scores, axis=1, keepdims=True)
        weights = jnp.exp(scores - tree_top)
        tree_total = jnp.sum(weights, axis=1, keepdims=True)
        arrived(s_v, r_v, v_send, v_recv)
        new_values = r_v[0].astype(F32)
        for i in range(1, NKV):
            new_values = new_values + r_v[i].astype(F32)
        new_values = (inverse * new_values).astype(BF16)
        tree_mix = diagonal(
            jnp.dot(weights.astype(BF16), new_values, preferred_element_type=F32), lane
        )
        tree_stats = stat_row(tree_top, tree_total)

        arrived(s_stat, r_stat, y_send, y_recv)
        stats = [r_stat[i] for i in range(NKV)] + [tree_stats]
        best = functools.reduce(jnp.maximum, stats)
        factors = [jnp.exp(s - best) for s in stats]
        denominator = functools.reduce(
            jnp.add,
            [pltpu.roll(s, COLS - HEADS * PROPS, 1) * f for s, f in zip(stats, factors)],
        )
        under = 1.0 / denominator
        shares = jnp.concatenate(
            [(f * under)[:, :LANES] for f in factors]
            + [jnp.zeros((LANES - NKV - 1, LANES), F32)],
            axis=0,
        )
        used = lax.broadcasted_iota(jnp.int32, shares.shape, 1) < HEADS * PROPS
        shares = jnp.where(used, shares, 0.0).T

        def share_of(i):
            return spread(
                [shares[h * PROPS : (h + 1) * PROPS, i : i + 1] for h in range(HEADS)], lane
            )

        attended = tree_mix * share_of(NKV)
        arrived(s_mix, r_mix, m_send, m_recv)
        for i in range(NKV):
            attended = attended + r_mix[i].astype(F32) * share_of(i)

        @pl.when(out_place != 1)
        def _():
            s_att[...] = attended.astype(BF16)

            for to in IN_ORDER:

                @pl.when((kv != to) | (tp != whole_to))
                def _():
                    whole_copy(to).start()

            @pl.when(tp == whole_to)
            def _():
                r_att[tp] = s_att[...]

        @pl.when(out_place == 1)
        def _():
            s_half[0] = attended[:HALF].astype(BF16)
            s_half[1] = attended[PROPS - HALF :].astype(BF16)

            for to in IN_ORDER:
                for c in range(2):

                    @pl.when((kv != to) | (tp != 2 * out_group + c))
                    def _():
                        half_copy(to, c).start()

            for c in range(2):

                @pl.when(tp == 2 * out_group + c)
                def _():
                    r_half[tp] = s_half[c]

    def scattered():
        @pl.when(is_owner)
        def _():
            sent_in_order()

    def sent_in_order():
        for to in IN_ORDER:

            @pl.when(is_whole & ((kv != to) | (tp != whole_to)))
            def _():
                whole_copy(to).wait_send()

            for c in range(2):

                @pl.when(is_half & ((kv != to) | (tp != 2 * out_group + c)))
                def _():
                    half_copy(to, c).wait_send()

    lax.fori_loop(1, NTP, weight_arrived, 0)
    for wait in pending:
        wait()

    for group in range(NTP):

        @pl.when((sources[0] != kv) | (tp != group))
        def _():
            pltpu.make_async_remote_copy(
                src_ref=s_att,
                dst_ref=r_att.at[group],
                send_sem=a_send.at[0],
                recv_sem=a_recv.at[group],
                device_id={"kv": sources[0], "tp": group},
                device_id_type=MESH,
            ).wait_recv()

        @pl.when((sources[1] != kv) | (tp != group))
        def _():
            pltpu.make_async_remote_copy(
                src_ref=s_half.at[0],
                dst_ref=r_half.at[group],
                send_sem=a_send.at[0],
                recv_sem=a_recv.at[NTP + group],
                device_id={"kv": sources[1], "tp": group},
                device_id_type=MESH,
            ).wait_recv()

    mixed = jnp.zeros((PROPS + HALF, COLS), F32)
    for group in range(NTP):
        whole, half = r_att[group].astype(F32), r_half[group].astype(F32)
        both = jnp.where(
            odd == 1,
            jnp.concatenate([half, whole], axis=0),
            jnp.concatenate([whole, half], axis=0),
        )
        term = jnp.dot(both.astype(BF16), v_wo[group], preferred_element_type=F32)
        mixed = mixed + term.astype(BF16).astype(F32)
    out_ref[...] = jnp.where(
        odd == 1, mixed[PROPS + HALF - OUT_ROWS :], mixed[:OUT_ROWS]
    ).astype(BF16)
    scattered()


def body(
    tokens,
    norm_gain,
    query_weight,
    key_weight,
    value_weight,
    gate_weight,
    gate_bias,
    out_weight,
    cache_keys,
    cache_values,
    cache_decay,
    lengths,
    parents,
):
    anywhere = pl.BlockSpec(memory_space=pl.ANY)
    vector = pl.BlockSpec(memory_space=pltpu.VMEM)
    dma = pltpu.SemaphoreType.DMA
    return pl.pallas_call(
        kernel,
        out_shape=jax.ShapeDtypeStruct((OUT_ROWS, COLS), BF16),
        in_specs=[anywhere] * 13,
        out_specs=vector,
        scratch_shapes=[
            pltpu.VMEM((ROWS, COLS), BF16),
            pltpu.VMEM((1, COLS), F32),
            pltpu.VMEM((COLS, COLS), BF16),
            pltpu.VMEM((COLS, COLS), BF16),
            pltpu.VMEM((COLS, COLS), BF16),
            pltpu.VMEM((32, COLS), BF16),
            pltpu.VMEM((NTP, COLS, COLS), BF16),
            pltpu.VMEM((SEQS, POS, COLS), BF16),
            pltpu.VMEM((SEQS, POS, COLS), BF16),
            pltpu.VMEM((SEQS, HEADS, POS), F32),
            pltpu.SMEM((SEQS,), jnp.int32),
            pltpu.SMEM((NTP * HEADS,), F32),
            pltpu.VMEM((SEQS, PROPS), jnp.int32),
            pltpu.VMEM((SEQS, PROPS, COLS), F32),
            pltpu.VMEM((SEQS, 1, LANES), F32),
            pltpu.VMEM((SEQS, PROPS, COLS), F32),
            pltpu.VMEM((SEQS, PROPS, COLS), BF16),
            pltpu.VMEM((NKV, PROPS, COLS), F32),
            pltpu.VMEM((NKV, 1, LANES), F32),
            pltpu.VMEM((NKV, PROPS, COLS), F32),
            pltpu.VMEM((NKV, PROPS, COLS), BF16),
            pltpu.VMEM((SEQS, PROPS, COLS), BF16),
            pltpu.VMEM((1, LANES), F32),
            pltpu.VMEM((PROPS, LANES), F32),
            pltpu.VMEM((SEQS, PROPS, COLS), BF16),
            pltpu.VMEM((SEQS, 1, COLS), F32),
            pltpu.VMEM((NKV, PROPS, COLS), BF16),
            pltpu.VMEM((NKV, 1, COLS), F32),
            pltpu.VMEM((PROPS, COLS), BF16),
            pltpu.VMEM((2, HALF, COLS), BF16),
            pltpu.VMEM((NTP, PROPS, COLS), BF16),
            pltpu.VMEM((NTP, HALF, COLS), BF16),
            dma((13,)),
            dma((SEQS,)),
            dma((NKV,)),
            dma((SEQS,)),
            dma((NKV,)),
            dma((SEQS,)),
            dma((NKV,)),
            dma((SEQS,)),
            dma((NKV,)),
            dma((NKV,)),
            dma((SEQS,)),
            dma((SEQS,)),
            dma((NKV,)),
            dma((SEQS,)),
            dma((NKV,)),
            dma((2 * NKV,)),
            dma((2 * NTP,)),
            dma((NTP,)),
            dma((NTP,)),
        ],
        compiler_params=pltpu.CompilerParams(
            collective_id=0, has_side_effects=True, vmem_limit_bytes=60 * 1024 * 1024
        ),
        name="tree_attention",
    )(
        tokens,
        norm_gain.reshape(1, -1),
        query_weight,
        key_weight,
        value_weight,
        gate_weight.T,
        gate_bias,
        out_weight,
        cache_keys,
        cache_values,
        cache_decay,
        lengths,
        parents,
    )


def solution(mesh):
    in_specs = (
        P(None, "kv"),
        P("kv"),
        P("kv", "tp"),
        P("kv", "tp"),
        P("kv", "tp"),
        P(),
        P(),
        P("tp", "kv"),
        P(None, "kv", "tp"),
        P(None, "kv", "tp"),
        P(None, "tp", "kv"),
        P(),
        P(),
    )
    out_specs = P("tp", "kv")
    return jax.shard_map(body, mesh=mesh, in_specs=in_specs, out_specs=out_specs, check_vma=False)
```
